32 devices in a mesh: kv: 8 (over z, x), tp: 4 (over y, core).
Axes of the slice: x: 2, y: 2, z: 4, core: 2. Of those that a mesh axis runs over, the one named last changes fastest.
Arguments:
- tokens: bfloat16 [64, 12, 4096], P(None, None, 'kv'), may hold values from -6 to 6
- parents: int32 [64, 12], P('kv'), may hold values from -1 to 10, as said below
- accepted: int32 [64], P('kv'), may hold values from 0 to 6
- state: float32 [64, 64, 64, 128], P('kv', 'tp'), may hold values from -4 to 4
- conv_x: bfloat16 [64, 3, 4096], P('kv', None, 'tp'), may hold values from -6 to 6
- conv_b: bfloat16 [64, 3, 2048], P('kv', None, 'tp'), may hold values from -6 to 6
- conv_c: bfloat16 [64, 3, 2048], P('kv', None, 'tp'), may hold values from -6 to 6
- path_x: bfloat16 [64, 6, 4096], P('kv', None, 'tp'), may hold values from -6 to 6
- path_b: bfloat16 [64, 6, 2048], P('kv', None, 'tp'), may hold values from -6 to 6
- path_c: bfloat16 [64, 6, 2048], P('kv', None, 'tp'), may hold values from -6 to 6
- path_dt: bfloat16 [64, 6, 64], P('kv', None, 'tp'), may hold values from -6 to 6
- gain_in: float32 [4096], replicated, may hold values from 0.1 to 1.9
- w_x: bfloat16 [4096, 4096], P('kv', 'tp'), may hold values from -0.09375 to 0.09375
- w_z: bfloat16 [4096, 4096], P('kv', 'tp'), may hold values from -0.09375 to 0.09375
- w_b: bfloat16 [4096, 2048], P('kv', 'tp'), may hold values from -0.09375 to 0.09375
- w_c: bfloat16 [4096, 2048], P('kv', 'tp'), may hold values from -0.09375 to 0.09375
- w_dt: bfloat16 [4096, 64], replicated, may hold values from -0.09375 to 0.09375
- dt_bias: float32 [64], P('tp'), may hold values from -2 to 1
- a_log: float32 [64], P('tp'), may hold values from -3 to 1.5
- d_skip: float32 [64], P('tp'), may hold values from 0.5 to 1.5
- conv_wx: bfloat16 [4, 4096], P(None, 'tp'), may hold values from -3 to 3
- conv_wb: bfloat16 [4, 2048], P(None, 'tp'), may hold values from -3 to 3
- conv_wc: bfloat16 [4, 2048], P(None, 'tp'), may hold values from -3 to 3
- gain_out: float32 [4096], P('tp'), may hold values from 0.1 to 1.9
- w_out: bfloat16 [4096, 4096], P('tp', 'kv'), may hold values from -0.09375 to 0.09375
Outputs:
- mixed: bfloat16 [64, 12, 4096], P('kv', None, 'tp')
- new_state: float32 [64, 64, 64, 128], P('kv', 'tp')
The draws below stay inside these ranges and needn't reach their ends.
Inputs may be any that keep to these rules, and one draw needn't show every extreme that they name: `parents`: each proposal's parent is -1 or an earlier proposal of the same sequence; the first proposal's parent is -1.
All inputs are finite; a program needn't handle non-finite values.
Results may differ from the reference program's by a relative error of at most 0.03.
Values may be sent and summed in bfloat16 or wider, within the bound.
A program may use at most 128 MiB of HBM per device.

```python
import jax
import jax.numpy as jnp
from jax import lax

D = 4096
G = 16
HPG = 4
H = 64
HD = 64
N = 128
INNER = 4096
CONV = 4
Q = 12
P_SIZE = 6
SEQS = 64
N_TP = 4


def draw_parents(key, part):
    jumps = jax.random.randint(key, (SEQS, Q), 0, 3)
    places = jnp.arange(Q, dtype=jnp.int32)[None, :]
    return jnp.maximum(places - 1 - jumps, -1).astype(jnp.int32)


def touch_ends(array, key, low, largest):
    longest = array.shape.index(max(array.shape))
    spots = []
    for shift in (0, 1):
        where = [jax.random.randint(jax.random.fold_in(key, axis), (), 0, length) for axis, length in enumerate(array.shape)]
        where[longest] = (where[longest] + shift) % array.shape[longest]
        spots.append(tuple(where))
    return array.at[spots[0]].set(low).at[spots[1]].set(largest)


def raised(values, stream_key, source, target, shards_of, factor):
    def block_of(position):
        return (jnp.arange(values.shape[position]) // (values.shape[position] // shards_of)).reshape((-1,) + (1,) * (values.ndim - 1 - position))

    near = jax.random.permutation(stream_key, shards_of)[block_of(target)]
    second = (block_of(target) + shards_of // 2) % shards_of
    return jnp.where((block_of(source) == near) | (block_of(source) == second), factor * values, values)


def block_scale(key, extent, split, smallest, high):
    gain = 1.0
    for dim, blocks in split:
        steps = jax.random.uniform(jax.random.fold_in(jax.random.fold_in(key, 6), dim), (blocks,), jnp.float32, smallest / len(split), high / len(split))
        gain = gain * jnp.repeat(jnp.exp(steps), extent[dim] // blocks).reshape((-1,) + (1,) * (len(extent) - 1 - dim))
    return gain


def noise(rng, dims, spread, bound, shards=(), kind=jnp.bfloat16):
    array = jax.random.normal(rng, dims, jnp.float32) * spread
    if len(shards) > 0:
        array = block_scale(rng, dims, shards, -0.22, 0.18) * array
    return jnp.clip(array, min=-bound, max=bound).astype(kind)


def heavy_noise(own_key, shape, deviation, reach, shards, heavy, kind=jnp.bfloat16):
    array = deviation * jax.random.normal(own_key, shape, jnp.float32)
    if shards:
        array = array * block_scale(own_key, shape, shards, -0.22, 0.18)
    return jnp.clip(raised(array, jax.random.fold_in(own_key, 3), *heavy), -reach, reach).astype(kind)


def setup_inputs(seed: int = 0) -> dict:
    key_list = jax.random.split(jax.random.key(seed), 26)
    tokens = heavy_noise(key_list[0], (SEQS, Q, D), 1.0, 6.0, ((2, 8),), (2, 0, 8, 2.0))
    parents = draw_parents(jax.random.fold_in(key_list[25], 71), 0)
    accepted = touch_ends(jax.random.randint(key_list[2], (SEQS,), 0, P_SIZE + 1), jax.random.fold_in(key_list[2], 1), 0, P_SIZE).astype(jnp.int32)
    state = noise(key_list[3], (SEQS, H, HD, N), 0.3, 4.0, ((0, 8), (1, 4)), jnp.float32)
    conv_x = noise(key_list[4], (SEQS, CONV - 1, INNER), 1.0, 6.0, ((0, 8), (2, 4)))
    conv_b = noise(key_list[5], (SEQS, CONV - 1, G * N), 1.0, 6.0, ((0, 8), (2, 4)))
    conv_c = noise(key_list[6], (SEQS, CONV - 1, G * N), 1.0, 6.0, ((0, 8), (2, 4)))
    path_x = noise(key_list[7], (SEQS, P_SIZE, INNER), 1.0, 6.0, ((0, 8), (2, 4)))
    path_b = noise(key_list[8], (SEQS, P_SIZE, G * N), 1.0, 6.0, ((0, 8), (2, 4)))
    path_c = noise(key_list[9], (SEQS, P_SIZE, G * N), 1.0, 6.0, ((0, 8), (2, 4)))
    path_dt = noise(key_list[10], (SEQS, P_SIZE, H), 1.0, 6.0, ((0, 8), (2, 4)))
    gain_in = jnp.clip(1.0 + 0.18 * jax.random.normal(key_list[11], (D,), jnp.float32), 0.1, 1.9)
    w_x = noise(key_list[12], (D, INNER), D ** -0.5, 0.09375, ((0, 8), (1, 4)))
    w_z = noise(key_list[13], (D, INNER), D ** -0.5, 0.09375, ((0, 8), (1, 4)))
    w_b = noise(key_list[14], (D, G * N), D ** -0.5, 0.09375, ((0, 8), (1, 4)))
    w_c = noise(key_list[15], (D, G * N), D ** -0.5, 0.09375, ((0, 8), (1, 4)))
    w_dt = noise(key_list[16], (D, H), D ** -0.5, 0.09375)
    dt_bias = jnp.clip(-2.0 + 3.0 * jax.random.uniform(key_list[17], (H,), jnp.float32) ** block_scale(key_list[17], (H,), ((0, 4),), -0.2, 0.2), -2.0, 1.0)
    a_log = jnp.clip(-3.0 + 4.5 * jax.random.uniform(key_list[18], (H,), jnp.float32) ** block_scale(key_list[18], (H,), ((0, 4),), -0.2, 0.2), -3.0, 1.5)
    d_skip = jnp.clip(0.5 + 1.0 * jax.random.uniform(key_list[19], (H,), jnp.float32) ** block_scale(key_list[19], (H,), ((0, 4),), -0.2, 0.2), 0.5, 1.5)
    conv_wx = noise(key_list[20], (CONV, INNER), 0.5, 3.0, ((1, 4),))
    conv_wb = noise(key_list[21], (CONV, G * N), 0.5, 3.0, ((1, 4),))
    conv_wc = noise(key_list[22], (CONV, G * N), 0.5, 3.0, ((1, 4),))
    gain_out = jnp.clip(1.0 + 0.18 * jax.random.normal(key_list[23], (INNER,), jnp.float32), 0.1, 1.9)
    w_out = noise(key_list[24], (INNER, D), INNER ** -0.5, 0.09375, ((0, 4), (1, 8)))
    return dict(tokens=tokens, parents=parents, accepted=accepted, state=state, conv_x=conv_x, conv_b=conv_b, conv_c=conv_c, path_x=path_x, path_b=path_b, path_c=path_c, path_dt=path_dt, gain_in=gain_in, w_x=w_x, w_z=w_z, w_b=w_b, w_c=w_c, w_dt=w_dt, dt_bias=dt_bias, a_log=a_log, d_skip=d_skip, conv_wx=conv_wx, conv_wb=conv_wb, conv_wc=conv_wc, gain_out=gain_out, w_out=w_out)


EPS = 1e-06
HIGH = lax.Precision.HIGHEST

def conv_window(history, taps, amount):
    values = history.astype(jnp.float32)
    weights = taps.astype(jnp.float32)
    summed = weights[0] * values[:, 0:amount, :]
    for distance in range(1, weights.shape[0]):
        summed = summed + weights[distance] * values[:, distance:distance + amount, :]
    return jax.nn.silu(summed)

def commit_rows(history, accepted, keep):
    picked = accepted[:, None].astype(jnp.int32) + jnp.arange(keep, dtype=jnp.int32)[None, :]
    select = (picked[:, :, None] == jnp.arange(history.shape[1], dtype=jnp.int32)[None, None, :]).astype(jnp.float32)
    return jnp.einsum('skl,slc->skc', select, history.astype(jnp.float32), precision=HIGH).astype(jnp.bfloat16)

def replay_state(state, history_x, history_b, path_dt, conv_wx, conv_wb, accepted, rate_bias, a_rate, per_group):
    seq_count, heads, head_dim, state_dim = state.shape
    path_len = path_dt.shape[1]
    path_xs = conv_window(history_x, conv_wx, path_len).reshape(seq_count, path_len, heads, head_dim)
    path_bs = conv_window(history_b, conv_wb, path_len).reshape(seq_count, path_len, heads // per_group, state_dim)
    path_bh = jnp.repeat(path_bs, per_group, axis=2)
    path_step = jax.nn.softplus(path_dt.astype(jnp.float32) + rate_bias)
    is_live = (jnp.arange(path_len, dtype=jnp.int32)[None, :] < accepted[:, None].astype(jnp.int32)).astype(jnp.float32)[:, :, None]
    log_decay = path_step * a_rate * is_live
    overall = lax.optimization_barrier(jnp.sum(log_decay, axis=1))
    tail_sum = overall[:, None, :] - jnp.cumsum(log_decay, axis=1)
    weights = is_live * jnp.exp(tail_sum) * path_step
    grown = jnp.einsum('sjh,sjhp,sjhn->shpn', weights, path_xs, path_bh, precision=HIGH)
    return jnp.exp(overall)[:, :, None, None] * state + grown

def tree_links(parents, keep):
    seq_count, prop_count = parents.shape
    front = jnp.broadcast_to(jnp.arange(-1, keep - 1, dtype=jnp.int32)[None, :], (seq_count, keep))
    parent_ids = jnp.concatenate([front, parents.astype(jnp.int32) + keep], axis=1)
    nodes = keep + prop_count
    links = (parent_ids[:, :, None] == jnp.arange(nodes, dtype=jnp.int32)[None, None, :]).astype(jnp.float32)
    identity = jnp.eye(prop_count, dtype=jnp.float32)[None, :, :]
    ancestry = identity + links[:, keep:, keep:]
    for turn in range(prop_count.bit_length()):
        ancestry = jnp.minimum(jnp.einsum('sij,sjk->sik', ancestry, ancestry, precision=HIGH), 1.0)
    return (links, ancestry)

def tree_conv(buffer, rows, taps, links, keep):
    values = jnp.concatenate([buffer, rows], axis=1).astype(jnp.float32)
    weights = taps.astype(jnp.float32)
    last_tap = weights.shape[0] - 1
    summed = weights[last_tap] * values
    reached = values
    for distance in range(1, last_tap + 1):
        reached = jnp.einsum('sij,sjc->sic', links, reached, precision=HIGH)
        summed = summed + weights[last_tap - distance] * reached
    return jax.nn.silu(summed[:, keep:, :])

def tree_mix(state, post_x, post_b, post_c, rate_rows, z_rows, ancestry, rate_bias, a_rate, d_skip, gain_out, per_group):
    seq_count, prop_count, _ = post_x.shape
    heads, head_dim, state_dim = (state.shape[1], state.shape[2], state.shape[3])
    groups = heads // per_group
    x_heads = post_x.reshape(seq_count, prop_count, heads, head_dim)
    b_groups = post_b.reshape(seq_count, prop_count, groups, state_dim)
    c_groups = post_c.reshape(seq_count, prop_count, groups, state_dim)
    step_size = jax.nn.softplus(rate_rows.astype(jnp.float32) + rate_bias)
    path_decay = jnp.einsum('sij,sjh->sih', ancestry, step_size * a_rate, precision=HIGH)
    c_heads = jnp.repeat(c_groups, per_group, axis=2)
    carried = jnp.einsum('sihn,shpn->sihp', c_heads, state, precision=HIGH) * jnp.exp(path_decay)[:, :, :, None]
    scores = jnp.einsum('sign,sjgn->sgij', c_groups, b_groups, precision=HIGH)
    scores = jnp.repeat(scores, per_group, axis=1)
    decay_t = jnp.transpose(path_decay, (0, 2, 1))
    decay_gap = decay_t[:, :, :, None] - decay_t[:, :, None, :]
    is_live = ancestry[:, None, :, :] > 0.5
    mixing = jnp.where(is_live, jnp.exp(jnp.where(is_live, decay_gap, 0.0)), 0.0)
    mixing = mixing * jnp.transpose(step_size, (0, 2, 1))[:, :, None, :]
    within = jnp.einsum('shij,sjhp->sihp', scores * mixing, x_heads, precision=HIGH)
    heads_out = carried + within + d_skip[None, None, :, None] * x_heads
    heads_out = heads_out.reshape(seq_count, prop_count, heads * head_dim) * jax.nn.silu(z_rows.astype(jnp.float32))
    grouped = heads_out.reshape(seq_count, prop_count, groups, per_group * head_dim)
    grouped = grouped * lax.rsqrt(lax.optimization_barrier(jnp.mean(grouped * grouped, axis=-1, keepdims=True)) + EPS)
    return (grouped.reshape(seq_count, prop_count, heads * head_dim) * gain_out).astype(jnp.bfloat16)

def reference(tokens, parents, accepted, state, conv_x, conv_b, conv_c, path_x, path_b, path_c, path_dt, gain_in, w_x, w_z, w_b, w_c, w_dt, dt_bias, a_log, d_skip, conv_wx, conv_wb, conv_wc, gain_out, w_out):
    seq_count, prop_count, width = tokens.shape
    keep = conv_wx.shape[0] - 1
    flat_rows = tokens.reshape(-1, width).astype(jnp.float32)
    row_scale = lax.rsqrt(lax.optimization_barrier(jnp.sum(flat_rows * flat_rows, axis=1)) / width + EPS)[:, None]
    scaled = (flat_rows * gain_in).astype(jnp.bfloat16)

    def project(weight):
        product = jnp.dot(scaled, weight, preferred_element_type=jnp.float32) * row_scale
        return product.astype(jnp.bfloat16).reshape(seq_count, prop_count, -1)
    x_rows = project(w_x)
    z_rows = project(w_z)
    b_rows = project(w_b)
    c_rows = project(w_c)
    rate_rows = project(w_dt)
    a_rate = -jnp.exp(a_log)
    history_x = jnp.concatenate([conv_x, path_x], axis=1)
    history_b = jnp.concatenate([conv_b, path_b], axis=1)
    history_c = jnp.concatenate([conv_c, path_c], axis=1)
    new_state = replay_state(state, history_x, history_b, path_dt, conv_wx, conv_wb, accepted, dt_bias, a_rate, HPG)
    links, ancestry = tree_links(parents, keep)
    post_x = tree_conv(commit_rows(history_x, accepted, keep), x_rows, conv_wx, links, keep)
    post_b = tree_conv(commit_rows(history_b, accepted, keep), b_rows, conv_wb, links, keep)
    post_c = tree_conv(commit_rows(history_c, accepted, keep), c_rows, conv_wc, links, keep)
    gated = tree_mix(new_state, post_x, post_b, post_c, rate_rows, z_rows, ancestry, dt_bias, a_rate, d_skip, gain_out, HPG)
    block = gated.shape[2] // N_TP
    gated_flat = gated.reshape(-1, gated.shape[2])
    running = jnp.zeros((gated_flat.shape[0], width), jnp.float32)
    for index in range(N_TP):
        term = jnp.dot(gated_flat[:, index * block:(index + 1) * block], w_out[index * block:(index + 1) * block, :], preferred_element_type=jnp.float32)
        rounded = lax.optimization_barrier(term.astype(jnp.bfloat16))
        running = running + rounded.astype(jnp.float32)
    mixed = running.astype(jnp.bfloat16).reshape(seq_count, prop_count, width)
    return (mixed, new_state)
```

```python
import functools

import jax
import jax.numpy as jnp
from jax import lax
from jax.experimental import pallas as pl
from jax.experimental.pallas import tpu as pltpu
from jax.sharding import PartitionSpec as P

HPG = 4


EPS = 1e-06
HIGH = lax.Precision.HIGHEST
MESH = pl.DeviceIdType.MESH


def scatter_kernel(
    ranks, width, square_column, part_ref, side_ref, rows_ref, rate_ref, got, got_side, sends, recvs
):
    mine = lax.axis_index("kv")
    column = lax.axis_index("tp")
    barrier = pltpu.get_barrier_semaphore()
    for offset in range(1, ranks):
        pl.semaphore_signal(
            barrier,
            inc=1,
            device_id=(lax.rem(mine + offset, ranks), column),
            device_id_type=MESH,
        )
    pl.semaphore_wait(barrier, ranks - 1)
    copies = []
    for offset in range(1, ranks):
        target = lax.rem(mine + offset, ranks)
        for which, (source, landing) in enumerate(((side_ref, got_side), (part_ref, got))):
            copy = pltpu.make_async_remote_copy(
                src_ref=source.at[target],
                dst_ref=landing.at[offset - 1],
                send_sem=sends.at[which, offset - 1],
                recv_sem=recvs.at[which, offset - 1],
                device_id=(target, column),
                device_id_type=MESH,
            )
            copy.start()
            copies.append(copy)
    for copy in copies:
        copy.wait()
    side = side_ref[mine].astype(jnp.float32)
    for offset in range(1, ranks):
        side = side + got_side[offset - 1].astype(jnp.float32)
    row_scale = lax.rsqrt(side[:, square_column : square_column + 1] / width + EPS)
    rate_ref[...] = (side * row_scale).astype(rate_ref.dtype)
    columns = rows_ref.shape[1]
    step = 512 if columns % 512 == 0 else columns

    @pl.loop(0, columns // step)
    def _(turn):
        span = pl.ds(pl.multiple_of(turn * step, step), step)
        total = part_ref[mine, :, span].astype(jnp.float32)
        for offset in range(1, ranks):
            total = total + got[offset - 1, :, span].astype(jnp.float32)
        rows_ref[:, span] = (total * row_scale).astype(rows_ref.dtype)


def scatter_rows(part, side, width, square_column):
    ranks, rows, columns = part.shape
    side_columns = side.shape[2]
    vmem = pl.BlockSpec(memory_space=pltpu.VMEM)
    return pl.pallas_call(
        functools.partial(scatter_kernel, ranks, width, square_column),
        out_shape=(
            jax.ShapeDtypeStruct((rows, columns), jnp.bfloat16),
            jax.ShapeDtypeStruct((rows, side_columns), jnp.bfloat16),
        ),
        in_specs=[vmem, vmem],
        out_specs=(vmem, vmem),
        scratch_shapes=[
            pltpu.VMEM((ranks - 1, rows, columns), jnp.bfloat16),
            pltpu.VMEM((ranks - 1, rows, side_columns), jnp.bfloat16),
            pltpu.SemaphoreType.DMA((2, ranks - 1)),
            pltpu.SemaphoreType.DMA((2, ranks - 1)),
        ],
        compiler_params=pltpu.CompilerParams(collective_id=0, has_side_effects=True),
    )(part, side)


def out_kernel(
    ranks,
    blocks,
    gated_ref,
    w_ref,
    mixed_ref,
    gathered,
    terms,
    landed,
    gather_sends,
    gather_recvs,
    term_sends,
    term_recvs,
):
    mine = lax.axis_index("kv")
    column = lax.axis_index("tp")
    ratio = ranks // blocks
    owner = mine // ratio
    place = lax.rem(mine, ratio)
    slab = w_ref.shape[1]
    barrier = pltpu.get_barrier_semaphore()
    for offset in range(1, ranks):
        pl.semaphore_signal(
            barrier,
            inc=1,
            device_id=(lax.rem(mine + offset, ranks), column),
            device_id_type=MESH,
        )
    for near in range(ratio):
        source = column * ratio + near
        for block in range(blocks):

            @pl.when(block != column)
            def _():
                pl.semaphore_signal(
                    barrier, inc=1, device_id=(source, block), device_id_type=MESH
                )

    @pl.when(owner == column)
    def _():
        pl.semaphore_wait(barrier, ranks - 1)

    @pl.when(owner != column)
    def _():
        pl.semaphore_wait(barrier, 2 * ranks - 1)

    copies = []
    for offset in range(1, ranks):
        copy = pltpu.make_async_remote_copy(
            src_ref=gated_ref,
            dst_ref=gathered.at[offset - 1],
            send_sem=gather_sends.at[offset - 1],
            recv_sem=gather_recvs.at[offset - 1],
            device_id=(lax.rem(mine + offset, ranks), column),
            device_id_type=MESH,
        )
        copy.start()
        copies.append(copy)

    def term_copy(offset, target):
        return pltpu.make_async_remote_copy(
            src_ref=terms.at[offset],
            dst_ref=landed.at[place, column],
            send_sem=term_sends.at[offset],
            recv_sem=term_recvs.at[place, column],
            device_id=(target, owner),
            device_id_type=MESH,
        )

    for offset in range(ranks):
        target = lax.rem(mine + ranks - offset, ranks)
        if offset == 0:
            block = gated_ref[...]
        else:
            copies[offset - 1].wait_recv()
            block = gathered[offset - 1]
        term = jnp.dot(block, w_ref[...], preferred_element_type=jnp.float32).astype(
            jnp.bfloat16
        )
        if offset == 0:

            @pl.when(owner == column)
            def _():
                landed[place, column] = term

            @pl.when(owner != column)
            def _():
                terms[0] = term
                term_copy(0, target).start()

        else:
            terms[offset] = term
            term_copy(offset, target).start()

    for near in range(ratio):
        source = column * ratio + near
        for block in range(blocks):

            @pl.when(jnp.logical_or(source != mine, block != column))
            def _():
                pltpu.make_async_remote_copy(
                    src_ref=terms.at[0],
                    dst_ref=landed.at[near, block],
                    send_sem=term_sends.at[0],
                    recv_sem=term_recvs.at[near, block],
                    device_id=(source, block),
                    device_id_type=MESH,
                ).wait_recv()

        total = landed[near, 0].astype(jnp.float32)
        for block in range(1, blocks):
            total = total + landed[near, block].astype(jnp.float32)
        mixed_ref[:, near * slab : (near + 1) * slab] = total.astype(mixed_ref.dtype)
    for offset in range(ranks):
        target = lax.rem(mine + ranks - offset, ranks)
        if offset == 0:

            @pl.when(owner != column)
            def _():
                term_copy(0, target).wait_send()

        else:
            copies[offset - 1].wait_send()
            term_copy(offset, target).wait_send()


def project_out(gated, w_out, ranks, blocks):
    rows = gated.shape[0]
    inner, slab = w_out.shape
    ratio = ranks // blocks
    vmem = pl.BlockSpec(memory_space=pltpu.VMEM)
    return pl.pallas_call(
        functools.partial(out_kernel, ranks, blocks),
        out_shape=jax.ShapeDtypeStruct((rows, ratio * slab), jnp.bfloat16),
        in_specs=[vmem, vmem],
        out_specs=vmem,
        scratch_shapes=[
            pltpu.VMEM((ranks - 1, rows, inner), jnp.bfloat16),
            pltpu.VMEM((ranks, rows, slab), jnp.bfloat16),
            pltpu.VMEM((ratio, blocks, rows, slab), jnp.bfloat16),
            pltpu.SemaphoreType.DMA((ranks - 1,)),
            pltpu.SemaphoreType.DMA((ranks - 1,)),
            pltpu.SemaphoreType.DMA((ranks,)),
            pltpu.SemaphoreType.DMA((ratio, blocks)),
        ],
        compiler_params=pltpu.CompilerParams(collective_id=1, has_side_effects=True),
    )(gated, w_out)


def conv_window(history, taps, amount):
    values = history.astype(jnp.float32)
    weights = taps.astype(jnp.float32)
    summed = weights[0] * values[:, 0:amount, :]
    for distance in range(1, weights.shape[0]):
        summed = summed + weights[distance] * values[:, distance : distance + amount, :]
    return jax.nn.silu(summed)


def commit_rows(history, accepted, keep):
    picked = accepted[:, None] + jnp.arange(keep, dtype=jnp.int32)[None, :]
    select = (
        picked[:, :, None] == jnp.arange(history.shape[1], dtype=jnp.int32)[None, None, :]
    ).astype(jnp.float32)
    return jnp.einsum("skl,slc->skc", select, history.astype(jnp.float32), precision=HIGH).astype(
        jnp.bfloat16
    )


def replay_state(
    state, history_x, history_b, path_dt, conv_wx, conv_wb, accepted, rate_bias, a_rate, per_group
):
    seq_count, heads, head_dim, state_dim = state.shape
    path_len = path_dt.shape[1]
    path_xs = conv_window(history_x, conv_wx, path_len).reshape(
        seq_count, path_len, heads, head_dim
    )
    path_bs = conv_window(history_b, conv_wb, path_len).reshape(
        seq_count, path_len, heads // per_group, state_dim
    )
    path_bh = jnp.repeat(path_bs, per_group, axis=2)
    path_step = jax.nn.softplus(path_dt.astype(jnp.float32) + rate_bias)
    is_live = (jnp.arange(path_len, dtype=jnp.int32)[None, :] < accepted[:, None]).astype(
        jnp.float32
    )[:, :, None]
    log_decay = path_step * a_rate * is_live
    overall = jnp.sum(log_decay, axis=1)
    tail_sum = overall[:, None, :] - jnp.cumsum(log_decay, axis=1)
    weights = is_live * jnp.exp(tail_sum) * path_step
    grown = jnp.einsum("sjh,sjhp,sjhn->shpn", weights, path_xs, path_bh, precision=HIGH)
    return jnp.exp(overall)[:, :, None, None] * state + grown


def tree_links(parents, keep):
    seq_count, prop_count = parents.shape
    front = jnp.broadcast_to(jnp.arange(-1, keep - 1, dtype=jnp.int32)[None, :], (seq_count, keep))
    parent_ids = jnp.concatenate([front, parents + keep], axis=1)
    nodes = keep + prop_count
    links = (parent_ids[:, :, None] == jnp.arange(nodes, dtype=jnp.int32)[None, None, :]).astype(
        jnp.float32
    )
    identity = jnp.eye(prop_count, dtype=jnp.float32)[None, :, :]
    ancestry = identity + links[:, keep:, keep:]
    for turn in range(prop_count.bit_length()):
        ancestry = jnp.minimum(jnp.einsum("sij,sjk->sik", ancestry, ancestry, precision=HIGH), 1.0)
    return (links, ancestry)


def tree_conv(buffer, rows, taps, links, keep):
    values = jnp.concatenate([buffer, rows], axis=1).astype(jnp.float32)
    weights = taps.astype(jnp.float32)
    last_tap = weights.shape[0] - 1
    summed = weights[last_tap] * values
    reached = values
    for distance in range(1, last_tap + 1):
        reached = jnp.einsum("sij,sjc->sic", links, reached, precision=HIGH)
        summed = summed + weights[last_tap - distance] * reached
    return jax.nn.silu(summed[:, keep:, :])


def tree_mix(
    state,
    post_x,
    post_b,
    post_c,
    rate_rows,
    z_rows,
    ancestry,
    rate_bias,
    a_rate,
    d_skip,
    gain_out,
    per_group,
):
    seq_count, prop_count, _ = post_x.shape
    heads, head_dim, state_dim = (state.shape[1], state.shape[2], state.shape[3])
    groups = heads // per_group
    x_heads = post_x.reshape(seq_count, prop_count, heads, head_dim)
    b_groups = post_b.reshape(seq_count, prop_count, groups, state_dim)
    c_groups = post_c.reshape(seq_count, prop_count, groups, state_dim)
    step_size = jax.nn.softplus(rate_rows.astype(jnp.float32) + rate_bias)
    path_decay = jnp.einsum("sij,sjh->sih", ancestry, step_size * a_rate, precision=HIGH)
    c_heads = jnp.repeat(c_groups, per_group, axis=2)
    carried = (
        jnp.einsum("sihn,shpn->sihp", c_heads, state, precision=HIGH)
        * jnp.exp(path_decay)[:, :, :, None]
    )
    scores = jnp.einsum("sign,sjgn->sgij", c_groups, b_groups, precision=HIGH)
    scores = jnp.repeat(scores, per_group, axis=1)
    decay_t = jnp.transpose(path_decay, (0, 2, 1))
    decay_gap = decay_t[:, :, :, None] - decay_t[:, :, None, :]
    is_live = ancestry[:, None, :, :] > 0.5
    mixing = jnp.where(is_live, jnp.exp(jnp.where(is_live, decay_gap, 0.0)), 0.0)
    mixing = mixing * jnp.transpose(step_size, (0, 2, 1))[:, :, None, :]
    within = jnp.einsum("shij,sjhp->sihp", scores * mixing, x_heads, precision=HIGH)
    heads_out = carried + within + d_skip[None, None, :, None] * x_heads
    heads_out = heads_out.reshape(seq_count, prop_count, heads * head_dim) * jax.nn.silu(
        z_rows.astype(jnp.float32)
    )
    grouped = heads_out.reshape(seq_count, prop_count, groups, per_group * head_dim)
    grouped = grouped * lax.rsqrt(jnp.mean(grouped * grouped, axis=-1, keepdims=True) + EPS)
    return (grouped.reshape(seq_count, prop_count, heads * head_dim) * gain_out).astype(
        jnp.bfloat16
    )


def shards(
    tokens,
    parents,
    accepted,
    state,
    conv_x,
    conv_b,
    conv_c,
    path_x,
    path_b,
    path_c,
    path_dt,
    gain_in,
    w_x,
    w_z,
    w_b,
    w_c,
    w_dt,
    dt_bias,
    a_log,
    d_skip,
    conv_wx,
    conv_wb,
    conv_wc,
    gain_out,
    w_out,
):
    seq_local = state.shape[0]
    proposals = parents.shape[1]
    heads_local = dt_bias.shape[0]
    inner_local = w_x.shape[1]
    group_cols = w_b.shape[1]
    width = gain_in.shape[0]
    keep = conv_wx.shape[0] - 1
    tp_index = lax.axis_index("tp")
    kv_index = lax.axis_index("kv")
    slab_width = tokens.shape[2]
    flat_rows = tokens.reshape(-1, slab_width).astype(jnp.float32)
    gain_part = lax.dynamic_slice_in_dim(gain_in, kv_index * slab_width, slab_width)
    scaled = (flat_rows * gain_part).astype(jnp.bfloat16)
    w_joined = jnp.concatenate([w_x, w_z, w_b, w_c], axis=1)
    ranks = lax.axis_size("kv")
    blocks = lax.axis_size("tp")
    part = jnp.dot(scaled, w_joined, preferred_element_type=jnp.float32).astype(jnp.bfloat16)
    w_rate = lax.dynamic_slice(
        w_dt, (kv_index * slab_width, tp_index * heads_local), (slab_width, heads_local)
    )
    rate_term = jnp.dot(scaled, w_rate, preferred_element_type=jnp.float32)
    squares = jnp.sum(flat_rows * flat_rows, axis=1, keepdims=True)
    side = jnp.concatenate([rate_term, squares], axis=1).astype(jnp.bfloat16)
    side = jnp.pad(side, ((0, 0), (0, -side.shape[1] % 128)))
    rows_all, rate_all = scatter_rows(
        part.reshape(ranks, -1, part.shape[1]),
        side.reshape(ranks, -1, side.shape[1]),
        width,
        heads_local,
    )

    def column_part(lower, upper):
        return rows_all[:, lower:upper].reshape(seq_local, proposals, upper - lower)

    x_rows = column_part(0, inner_local)
    z_rows = column_part(inner_local, 2 * inner_local)
    b_rows = column_part(2 * inner_local, 2 * inner_local + group_cols)
    c_rows = column_part(2 * inner_local + group_cols, 2 * inner_local + 2 * group_cols)
    rate_rows = rate_all[:, :heads_local].reshape(seq_local, proposals, heads_local)
    a_rate = -jnp.exp(a_log)
    history_x = jnp.concatenate([conv_x, path_x], axis=1)
    history_b = jnp.concatenate([conv_b, path_b], axis=1)
    history_c = jnp.concatenate([conv_c, path_c], axis=1)
    new_state = replay_state(
        state, history_x, history_b, path_dt, conv_wx, conv_wb, accepted, dt_bias, a_rate, HPG
    )
    links, ancestry = tree_links(parents, keep)
    post_x = tree_conv(commit_rows(history_x, accepted, keep), x_rows, conv_wx, links, keep)
    post_b = tree_conv(commit_rows(history_b, accepted, keep), b_rows, conv_wb, links, keep)
    post_c = tree_conv(commit_rows(history_c, accepted, keep), c_rows, conv_wc, links, keep)
    gated = tree_mix(
        new_state,
        post_x,
        post_b,
        post_c,
        rate_rows,
        z_rows,
        ancestry,
        dt_bias,
        a_rate,
        d_skip,
        gain_out,
        HPG,
    )
    gated_flat = gated.reshape(-1, inner_local)
    summed = project_out(gated_flat, w_out, ranks, blocks)
    mixed = summed.reshape(seq_local, proposals, -1)
    return (mixed, new_state)


def solution(mesh):
    return jax.shard_map(
        shards,
        mesh=mesh,
        in_specs=(
            P(None, None, "kv"),
            P("kv", None),
            P("kv"),
            P("kv", "tp", None, None),
            P("kv", None, "tp"),
            P("kv", None, "tp"),
            P("kv", None, "tp"),
            P("kv", None, "tp"),
            P("kv", None, "tp"),
            P("kv", None, "tp"),
            P("kv", None, "tp"),
            P(),
            P("kv", "tp"),
            P("kv", "tp"),
            P("kv", "tp"),
            P("kv", "tp"),
            P(),
            P("tp"),
            P("tp"),
            P("tp"),
            P(None, "tp"),
            P(None, "tp"),
            P(None, "tp"),
            P("tp"),
            P("tp", "kv"),
        ),
        out_specs=(P("kv", None, "tp"), P("kv", "tp", None, None)),
        check_vma=False,
    )
```

```python
import functools

import jax
import jax.numpy as jnp
from jax import lax
from jax.experimental import pallas as pl
from jax.experimental.pallas import tpu as pltpu
from jax.sharding import PartitionSpec as P

HPG = 4


EPS = 1e-06
HIGH = lax.Precision.HIGHEST
MESH = pl.DeviceIdType.MESH


def inner_size(ranks):
    return max(d for d in range(1, ranks + 1) if ranks % d == 0 and d * d <= ranks)


def scatter_kernel(
    near,
    far,
    width,
    square_column,
    part_ref,
    side_ref,
    rows_ref,
    rate_ref,
    near_main,
    near_side,
    sum_main,
    sum_side,
    far_main,
    far_side,
    near_sends,
    near_recvs,
    far_sends,
    far_recvs,
):
    mine = lax.axis_index("kv")
    column = lax.axis_index("tp")
    my_far = mine // near
    my_near = lax.rem(mine, near)

    def place(step_far, step_near):
        return lax.rem(my_far + step_far, far) * near + lax.rem(my_near + step_near, near)

    barrier = pltpu.get_barrier_semaphore()
    for step in range(1, near):
        pl.semaphore_signal(
            barrier, inc=1, device_id=(place(0, step), column), device_id_type=MESH
        )
    for step in range(1, far):
        pl.semaphore_signal(
            barrier, inc=1, device_id=(place(step, 0), column), device_id_type=MESH
        )
    pl.semaphore_wait(barrier, near + far - 2)
    order = list(range(1, far)) + [0]
    near_copies = {}
    for step_far in order:
        for step in range(1, near):
            for which, (source, landing) in enumerate(
                ((side_ref, near_side), (part_ref, near_main))
            ):
                copy = pltpu.make_async_remote_copy(
                    src_ref=source.at[place(step_far, step)],
                    dst_ref=landing.at[step_far, step - 1],
                    send_sem=near_sends.at[which, step_far, step - 1],
                    recv_sem=near_recvs.at[which, step_far, step - 1],
                    device_id=(place(0, step), column),
                    device_id_type=MESH,
                )
                copy.start()
                near_copies[step_far, step, which] = copy
    columns = rows_ref.shape[1]
    chunk = 512 if columns % 512 == 0 else columns
    far_copies = []
    for step_far in order:
        for step in range(1, near):
            for which in range(2):
                near_copies[step_far, step, which].wait_recv()
        if step_far == 0:
            break
        block = place(step_far, 0)
        side = side_ref[block].astype(jnp.float32)
        for step in range(1, near):
            side = side + near_side[step_far, step - 1].astype(jnp.float32)
        sum_side[step_far - 1] = side.astype(sum_side.dtype)

        @pl.loop(0, columns // chunk)
        def _(turn):
            span = pl.ds(pl.multiple_of(turn * chunk, chunk), chunk)
            total = part_ref[block, :, span].astype(jnp.float32)
            for step in range(1, near):
                total = total + near_main[step_far, step - 1, :, span].astype(jnp.float32)
            sum_main[step_far - 1, :, span] = total.astype(sum_main.dtype)

        for which, (source, landing) in enumerate(((sum_side, far_side), (sum_main, far_main))):
            copy = pltpu.make_async_remote_copy(
                src_ref=source.at[step_far - 1],
                dst_ref=landing.at[step_far - 1],
                send_sem=far_sends.at[which, step_far - 1],
                recv_sem=far_recvs.at[which, step_far - 1],
                device_id=(block, column),
                device_id_type=MESH,
            )
            copy.start()
            far_copies.append(copy)
    for copy in far_copies:
        copy.wait()
    for copy in near_copies.values():
        copy.wait_send()
    side = side_ref[mine].astype(jnp.float32)
    for step in range(1, near):
        side = side + near_side[0, step - 1].astype(jnp.float32)
    for step in range(1, far):
        side = side + far_side[step - 1].astype(jnp.float32)
    row_scale = lax.rsqrt(side[:, square_column : square_column + 1] / width + EPS)
    rate_ref[...] = (side * row_scale).astype(rate_ref.dtype)

    @pl.loop(0, columns // chunk)
    def _(turn):
        span = pl.ds(pl.multiple_of(turn * chunk, chunk), chunk)
        total = part_ref[mine, :, span].astype(jnp.float32)
        for step in range(1, near):
            total = total + near_main[0, step - 1, :, span].astype(jnp.float32)
        for step in range(1, far):
            total = total + far_main[step - 1, :, span].astype(jnp.float32)
        rows_ref[:, span] = (total * row_scale).astype(rows_ref.dtype)


def scatter_rows(part, side, width, square_column):
    ranks, rows, columns = part.shape
    side_columns = side.shape[2]
    near = inner_size(ranks)
    far = ranks // near
    vmem = pl.BlockSpec(memory_space=pltpu.VMEM)
    return pl.pallas_call(
        functools.partial(scatter_kernel, near, far, width, square_column),
        out_shape=(
            jax.ShapeDtypeStruct((rows, columns), jnp.bfloat16),
            jax.ShapeDtypeStruct((rows, side_columns), jnp.bfloat16),
        ),
        in_specs=[vmem, vmem],
        out_specs=(vmem, vmem),
        scratch_shapes=[
            pltpu.VMEM((far, near - 1, rows, columns), jnp.bfloat16),
            pltpu.VMEM((far, near - 1, rows, side_columns), jnp.bfloat16),
            pltpu.VMEM((far - 1, rows, columns), jnp.bfloat16),
            pltpu.VMEM((far - 1, rows, side_columns), jnp.bfloat16),
            pltpu.VMEM((far - 1, rows, columns), jnp.bfloat16),
            pltpu.VMEM((far - 1, rows, side_columns), jnp.bfloat16),
            pltpu.SemaphoreType.DMA((2, far, near - 1)),
            pltpu.SemaphoreType.DMA((2, far, near - 1)),
            pltpu.SemaphoreType.DMA((2, far - 1)),
            pltpu.SemaphoreType.DMA((2, far - 1)),
        ],
        compiler_params=pltpu.CompilerParams(collective_id=0, has_side_effects=True),
    )(part, side)


def out_kernel(
    ranks,
    blocks,
    gated_ref,
    w_ref,
    mixed_ref,
    gathered,
    terms,
    landed,
    gather_sends,
    gather_recvs,
    term_sends,
    term_recvs,
):
    mine = lax.axis_index("kv")
    column = lax.axis_index("tp")
    ratio = ranks // blocks
    owner = mine // ratio
    place = lax.rem(mine, ratio)
    slab = w_ref.shape[1]
    barrier = pltpu.get_barrier_semaphore()
    for offset in range(1, ranks):
        pl.semaphore_signal(
            barrier,
            inc=1,
            device_id=(lax.rem(mine + offset, ranks), column),
            device_id_type=MESH,
        )
    for near in range(ratio):
        source = column * ratio + near
        for block in range(blocks):

            @pl.when(block != column)
            def _():
                pl.semaphore_signal(
                    barrier, inc=1, device_id=(source, block), device_id_type=MESH
                )

    @pl.when(owner == column)
    def _():
        pl.semaphore_wait(barrier, ranks - 1)

    @pl.when(owner != column)
    def _():
        pl.semaphore_wait(barrier, 2 * ranks - 1)

    inner = inner_size(ranks)
    outer = ranks // inner
    my_outer = mine // inner
    my_inner = lax.rem(mine, inner)

    def spot(step_outer, step_inner):
        return lax.rem(my_outer + step_outer, outer) * inner + lax.rem(
            my_inner + step_inner, inner
        )

    copies = {}

    def gather_copy(source, offset, target):
        copy = pltpu.make_async_remote_copy(
            src_ref=source,
            dst_ref=gathered.at[offset - 1],
            send_sem=gather_sends.at[offset - 1],
            recv_sem=gather_recvs.at[offset - 1],
            device_id=(target, column),
            device_id_type=MESH,
        )
        copy.start()
        copies[offset] = copy

    for step in range(1, outer):
        gather_copy(gated_ref, step * inner, spot(step, 0))
    for step in range(1, inner):
        gather_copy(gated_ref, step, spot(0, step))

    def term_copy(offset, target):
        return pltpu.make_async_remote_copy(
            src_ref=terms.at[offset],
            dst_ref=landed.at[place, column],
            send_sem=term_sends.at[offset],
            recv_sem=term_recvs.at[place, column],
            device_id=(target, owner),
            device_id_type=MESH,
        )

    def origin(offset):
        return spot(outer - offset // inner, inner - offset % inner)

    turns = [0] + [step * inner for step in range(1, outer)]
    turns = turns + [offset for offset in range(ranks) if offset % inner]
    for offset in turns:
        target = origin(offset)
        if offset == 0:
            block = gated_ref[...]
        else:
            copies[offset].wait_recv()
            if offset % inner == 0:
                for step in range(1, inner):
                    gather_copy(gathered.at[offset - 1], offset + step, spot(0, step))
            block = gathered[offset - 1]
        term = jnp.dot(block, w_ref[...], preferred_element_type=jnp.float32).astype(
            jnp.bfloat16
        )
        if offset == 0:

            @pl.when(owner == column)
            def _():
                landed[place, column] = term

            @pl.when(owner != column)
            def _():
                terms[0] = term
                term_copy(0, target).start()

        else:
            terms[offset] = term
            term_copy(offset, target).start()

    for near in range(ratio):
        source = column * ratio + near
        for block in range(blocks):

            @pl.when(jnp.logical_or(source != mine, block != column))
            def _():
                pltpu.make_async_remote_copy(
                    src_ref=terms.at[0],
                    dst_ref=landed.at[near, block],
                    send_sem=term_sends.at[0],
                    recv_sem=term_recvs.at[near, block],
                    device_id=(source, block),
                    device_id_type=MESH,
                ).wait_recv()

        total = landed[near, 0].astype(jnp.float32)
        for block in range(1, blocks):
            total = total + landed[near, block].astype(jnp.float32)
        mixed_ref[:, near * slab : (near + 1) * slab] = total.astype(mixed_ref.dtype)
    for offset in range(ranks):
        target = origin(offset)
        if offset == 0:

            @pl.when(owner != column)
            def _():
                term_copy(0, target).wait_send()

        else:
            copies[offset].wait_send()
            term_copy(offset, target).wait_send()


def project_out(gated, w_out, ranks, blocks):
    rows = gated.shape[0]
    inner, slab = w_out.shape
    ratio = ranks // blocks
    vmem = pl.BlockSpec(memory_space=pltpu.VMEM)
    return pl.pallas_call(
        functools.partial(out_kernel, ranks, blocks),
        out_shape=jax.ShapeDtypeStruct((rows, ratio * slab), jnp.bfloat16),
        in_specs=[vmem, vmem],
        out_specs=vmem,
        scratch_shapes=[
            pltpu.VMEM((ranks - 1, rows, inner), jnp.bfloat16),
            pltpu.VMEM((ranks, rows, slab), jnp.bfloat16),
            pltpu.VMEM((ratio, blocks, rows, slab), jnp.bfloat16),
            pltpu.SemaphoreType.DMA((ranks - 1,)),
            pltpu.SemaphoreType.DMA((ranks - 1,)),
            pltpu.SemaphoreType.DMA((ranks,)),
            pltpu.SemaphoreType.DMA((ratio, blocks)),
        ],
        compiler_params=pltpu.CompilerParams(collective_id=1, has_side_effects=True),
    )(gated, w_out)


def conv_window(history, taps, amount):
    values = history.astype(jnp.float32)
    weights = taps.astype(jnp.float32)
    summed = weights[0] * values[:, 0:amount, :]
    for distance in range(1, weights.shape[0]):
        summed = summed + weights[distance] * values[:, distance : distance + amount, :]
    return jax.nn.silu(summed)


def commit_rows(history, accepted, keep):
    picked = accepted[:, None] + jnp.arange(keep, dtype=jnp.int32)[None, :]
    select = (
        picked[:, :, None] == jnp.arange(history.shape[1], dtype=jnp.int32)[None, None, :]
    ).astype(jnp.float32)
    return jnp.einsum("skl,slc->skc", select, history.astype(jnp.float32), precision=HIGH).astype(
        jnp.bfloat16
    )


def replay_state(
    state, history_x, history_b, path_dt, conv_wx, conv_wb, accepted, rate_bias, a_rate, per_group
):
    seq_count, heads, head_dim, state_dim = state.shape
    path_len = path_dt.shape[1]
    path_xs = conv_window(history_x, conv_wx, path_len).reshape(
        seq_count, path_len, heads, head_dim
    )
    path_bs = conv_window(history_b, conv_wb, path_len).reshape(
        seq_count, path_len, heads // per_group, state_dim
    )
    path_bh = jnp.repeat(path_bs, per_group, axis=2)
    path_step = jax.nn.softplus(path_dt.astype(jnp.float32) + rate_bias)
    is_live = (jnp.arange(path_len, dtype=jnp.int32)[None, :] < accepted[:, None]).astype(
        jnp.float32
    )[:, :, None]
    log_decay = path_step * a_rate * is_live
    overall = jnp.sum(log_decay, axis=1)
    tail_sum = overall[:, None, :] - jnp.cumsum(log_decay, axis=1)
    weights = is_live * jnp.exp(tail_sum) * path_step
    grown = jnp.einsum("sjh,sjhp,sjhn->shpn", weights, path_xs, path_bh, precision=HIGH)
    return jnp.exp(overall)[:, :, None, None] * state + grown


def tree_links(parents, keep):
    seq_count, prop_count = parents.shape
    front = jnp.broadcast_to(jnp.arange(-1, keep - 1, dtype=jnp.int32)[None, :], (seq_count, keep))
    parent_ids = jnp.concatenate([front, parents + keep], axis=1)
    nodes = keep + prop_count
    links = (parent_ids[:, :, None] == jnp.arange(nodes, dtype=jnp.int32)[None, None, :]).astype(
        jnp.float32
    )
    identity = jnp.eye(prop_count, dtype=jnp.float32)[None, :, :]
    ancestry = identity + links[:, keep:, keep:]
    for turn in range(prop_count.bit_length()):
        ancestry = jnp.minimum(jnp.einsum("sij,sjk->sik", ancestry, ancestry, precision=HIGH), 1.0)
    return (links, ancestry)


def tree_conv(buffer, rows, taps, links, keep):
    values = jnp.concatenate([buffer, rows], axis=1).astype(jnp.float32)
    weights = taps.astype(jnp.float32)
    last_tap = weights.shape[0] - 1
    summed = weights[last_tap] * values
    reached = values
    for distance in range(1, last_tap + 1):
        reached = jnp.einsum("sij,sjc->sic", links, reached, precision=HIGH)
        summed = summed + weights[last_tap - distance] * reached
    return jax.nn.silu(summed[:, keep:, :])


def tree_mix(
    state,
    post_x,
    post_b,
    post_c,
    rate_rows,
    z_rows,
    ancestry,
    rate_bias,
    a_rate,
    d_skip,
    gain_out,
    per_group,
):
    seq_count, prop_count, _ = post_x.shape
    heads, head_dim, state_dim = (state.shape[1], state.shape[2], state.shape[3])
    groups = heads // per_group
    x_heads = post_x.reshape(seq_count, prop_count, heads, head_dim)
    b_groups = post_b.reshape(seq_count, prop_count, groups, state_dim)
    c_groups = post_c.reshape(seq_count, prop_count, groups, state_dim)
    step_size = jax.nn.softplus(rate_rows.astype(jnp.float32) + rate_bias)
    path_decay = jnp.einsum("sij,sjh->sih", ancestry, step_size * a_rate, precision=HIGH)
    c_heads = jnp.repeat(c_groups, per_group, axis=2)
    carried = (
        jnp.einsum("sihn,shpn->sihp", c_heads, state, precision=HIGH)
        * jnp.exp(path_decay)[:, :, :, None]
    )
    scores = jnp.einsum("sign,sjgn->sgij", c_groups, b_groups, precision=HIGH)
    scores = jnp.repeat(scores, per_group, axis=1)
    decay_t = jnp.transpose(path_decay, (0, 2, 1))
    decay_gap = decay_t[:, :, :, None] - decay_t[:, :, None, :]
    is_live = ancestry[:, None, :, :] > 0.5
    mixing = jnp.where(is_live, jnp.exp(jnp.where(is_live, decay_gap, 0.0)), 0.0)
    mixing = mixing * jnp.transpose(step_size, (0, 2, 1))[:, :, None, :]
    within = jnp.einsum("shij,sjhp->sihp", scores * mixing, x_heads, precision=HIGH)
    heads_out = carried + within + d_skip[None, None, :, None] * x_heads
    heads_out = heads_out.reshape(seq_count, prop_count, heads * head_dim) * jax.nn.silu(
        z_rows.astype(jnp.float32)
    )
    grouped = heads_out.reshape(seq_count, prop_count, groups, per_group * head_dim)
    grouped = grouped * lax.rsqrt(jnp.mean(grouped * grouped, axis=-1, keepdims=True) + EPS)
    return (grouped.reshape(seq_count, prop_count, heads * head_dim) * gain_out).astype(
        jnp.bfloat16
    )


def shards(
    tokens,
    parents,
    accepted,
    state,
    conv_x,
    conv_b,
    conv_c,
    path_x,
    path_b,
    path_c,
    path_dt,
    gain_in,
    w_x,
    w_z,
    w_b,
    w_c,
    w_dt,
    dt_bias,
    a_log,
    d_skip,
    conv_wx,
    conv_wb,
    conv_wc,
    gain_out,
    w_out,
):
    seq_local = state.shape[0]
    proposals = parents.shape[1]
    heads_local = dt_bias.shape[0]
    inner_local = w_x.shape[1]
    group_cols = w_b.shape[1]
    width = gain_in.shape[0]
    keep = conv_wx.shape[0] - 1
    tp_index = lax.axis_index("tp")
    kv_index = lax.axis_index("kv")
    slab_width = tokens.shape[2]
    flat_rows = tokens.reshape(-1, slab_width).astype(jnp.float32)
    gain_part = lax.dynamic_slice_in_dim(gain_in, kv_index * slab_width, slab_width)
    scaled = (flat_rows * gain_part).astype(jnp.bfloat16)
    w_joined = jnp.concatenate([w_x, w_z, w_b, w_c], axis=1)
    ranks = lax.axis_size("kv")
    blocks = lax.axis_size("tp")
    part = jnp.dot(scaled, w_joined, preferred_element_type=jnp.float32).astype(jnp.bfloat16)
    w_rate = lax.dynamic_slice(
        w_dt, (kv_index * slab_width, tp_index * heads_local), (slab_width, heads_local)
    )
    rate_term = jnp.dot(scaled, w_rate, preferred_element_type=jnp.float32)
    squares = jnp.sum(flat_rows * flat_rows, axis=1, keepdims=True)
    side = jnp.concatenate([rate_term, squares], axis=1).astype(jnp.bfloat16)
    side = jnp.pad(side, ((0, 0), (0, -side.shape[1] % 128)))
    rows_all, rate_all = scatter_rows(
        part.reshape(ranks, -1, part.shape[1]),
        side.reshape(ranks, -1, side.shape[1]),
        width,
        heads_local,
    )

    def column_part(lower, upper):
        return rows_all[:, lower:upper].reshape(seq_local, proposals, upper - lower)

    x_rows = column_part(0, inner_local)
    z_rows = column_part(inner_local, 2 * inner_local)
    b_rows = column_part(2 * inner_local, 2 * inner_local + group_cols)
    c_rows = column_part(2 * inner_local + group_cols, 2 * inner_local + 2 * group_cols)
    rate_rows = rate_all[:, :heads_local].reshape(seq_local, proposals, heads_local)
    a_rate = -jnp.exp(a_log)
    history_x = jnp.concatenate([conv_x, path_x], axis=1)
    history_b = jnp.concatenate([conv_b, path_b], axis=1)
    history_c = jnp.concatenate([conv_c, path_c], axis=1)
    new_state = replay_state(
        state, history_x, history_b, path_dt, conv_wx, conv_wb, accepted, dt_bias, a_rate, HPG
    )
    links, ancestry = tree_links(parents, keep)
    post_x = tree_conv(commit_rows(history_x, accepted, keep), x_rows, conv_wx, links, keep)
    post_b = tree_conv(commit_rows(history_b, accepted, keep), b_rows, conv_wb, links, keep)
    post_c = tree_conv(commit_rows(history_c, accepted, keep), c_rows, conv_wc, links, keep)
    gated = tree_mix(
        new_state,
        post_x,
        post_b,
        post_c,
        rate_rows,
        z_rows,
        ancestry,
        dt_bias,
        a_rate,
        d_skip,
        gain_out,
        HPG,
    )
    gated_flat = gated.reshape(-1, inner_local)
    summed = project_out(gated_flat, w_out, ranks, blocks)
    mixed = summed.reshape(seq_local, proposals, -1)
    return (mixed, new_state)


def solution(mesh):
    return jax.shard_map(
        shards,
        mesh=mesh,
        in_specs=(
            P(None, None, "kv"),
            P("kv", None),
            P("kv"),
            P("kv", "tp", None, None),
            P("kv", None, "tp"),
            P("kv", None, "tp"),
            P("kv", None, "tp"),
            P("kv", None, "tp"),
            P("kv", None, "tp"),
            P("kv", None, "tp"),
            P("kv", None, "tp"),
            P(),
            P("kv", "tp"),
            P("kv", "tp"),
            P("kv", "tp"),
            P("kv", "tp"),
            P(),
            P("tp"),
            P("tp"),
            P("tp"),
            P(None, "tp"),
            P(None, "tp"),
            P(None, "tp"),
            P("tp"),
            P("tp", "kv"),
        ),
        out_specs=(P("kv", None, "tp"), P("kv", "tp", None, None)),
        check_vma=False,
    )
```

```python
import functools

import jax
import jax.numpy as jnp
from jax import lax
from jax.experimental import pallas as pl
from jax.experimental.pallas import tpu as pltpu
from jax.sharding import PartitionSpec as P

HPG = 4


EPS = 1e-06
HIGH = lax.Precision.HIGHEST
MESH = pl.DeviceIdType.MESH


def inner_size(ranks):
    return max(d for d in range(1, ranks + 1) if ranks % d == 0 and d * d <= ranks)


def scatter_kernel(
    near,
    far,
    width,
    square_column,
    part_ref,
    side_ref,
    rows_ref,
    rate_ref,
    near_main,
    near_side,
    sum_main,
    sum_side,
    pair_main,
    pair_side,
    pass_main,
    pass_side,
    far_main,
    far_side,
    near_sends,
    near_recvs,
    pair_sends,
    pair_recvs,
    far_sends,
    far_recvs,
):
    mine = lax.axis_index("kv")
    column = lax.axis_index("tp")
    my_far = mine // near
    my_near = lax.rem(mine, near)
    partner = my_far + 1 - 2 * lax.rem(my_far, 2)
    half = far // 2

    def place(home, jump, step_near):
        return lax.rem(home + 2 * jump, far) * near + lax.rem(my_near + step_near, near)

    barrier = pltpu.get_barrier_semaphore()
    peers = [place(my_far, 0, step) for step in range(1, near)]
    peers = peers + [place(partner, 0, 0)]
    peers = peers + [place(my_far, jump, 0) for jump in range(1, half)]
    for peer in peers:
        pl.semaphore_signal(barrier, inc=1, device_id=(peer, column), device_id_type=MESH)
    pl.semaphore_wait(barrier, len(peers))

    order = [(jump, kind) for jump in list(range(1, half)) + [0] for kind in range(2)]
    homes = (partner, my_far)
    near_copies = {}
    for jump, kind in order:
        slot = 2 * jump + kind
        for step in range(1, near):
            for which, (source, landing) in enumerate(
                ((side_ref, near_side), (part_ref, near_main))
            ):
                copy = pltpu.make_async_remote_copy(
                    src_ref=source.at[place(homes[kind], jump, step)],
                    dst_ref=landing.at[slot, step - 1],
                    send_sem=near_sends.at[which, slot, step - 1],
                    recv_sem=near_recvs.at[which, slot, step - 1],
                    device_id=(place(my_far, 0, step), column),
                    device_id_type=MESH,
                )
                copy.start()
                near_copies[slot, step, which] = copy
    columns = rows_ref.shape[1]
    chunk = 512 if columns % 512 == 0 else columns

    def add_up(block, slot, extra_main, extra_side, put_side, put_main):
        side = side_ref[block].astype(jnp.float32)
        for step in range(1, near):
            side = side + near_side[slot, step - 1].astype(jnp.float32)
        for ref, place_of in extra_side:
            side = side + ref[place_of].astype(jnp.float32)
        state = put_side(side)

        @pl.loop(0, columns // chunk)
        def _(turn):
            span = pl.ds(pl.multiple_of(turn * chunk, chunk), chunk)
            total = part_ref[block, :, span].astype(jnp.float32)
            for step in range(1, near):
                total = total + near_main[slot, step - 1, :, span].astype(jnp.float32)
            for ref, place_of in extra_main:
                total = total + ref[place_of, :, span].astype(jnp.float32)
            put_main(span, total, state)

    def send(refs, sems, source_at, target):
        made = []
        for which, (source, landing) in enumerate(refs):
            copy = pltpu.make_async_remote_copy(
                src_ref=source.at[source_at],
                dst_ref=landing.at[source_at],
                send_sem=sems[0].at[which, source_at],
                recv_sem=sems[1].at[which, source_at],
                device_id=(target, column),
                device_id_type=MESH,
            )
            copy.start()
            made.append(copy)
        return made

    def keep_side(ref, at):
        def put(side):
            ref[at] = side.astype(ref.dtype)

        return put

    def keep_main(ref, at):
        def put(span, total, state):
            ref[at, :, span] = total.astype(ref.dtype)

        return put

    pair_copies = {}
    far_copies = []
    for jump, kind in order:
        slot = 2 * jump + kind
        for step in range(1, near):
            for which in range(2):
                near_copies[slot, step, which].wait_recv()
        if kind == 0:
            add_up(
                place(partner, jump, 0),
                slot,
                [],
                [],
                keep_side(sum_side, jump),
                keep_main(sum_main, jump),
            )
            pair_copies[jump] = send(
                ((sum_side, pair_side), (sum_main, pair_main)),
                (pair_sends, pair_recvs),
                jump,
                place(partner, 0, 0),
            )
            continue
        for copy in pair_copies[jump]:
            copy.wait_recv()
        if jump > 0:
            target = place(my_far, jump, 0)
            add_up(
                target,
                slot,
                [(pair_main, jump)],
                [(pair_side, jump)],
                keep_side(pass_side, jump - 1),
                keep_main(pass_main, jump - 1),
            )
            far_copies = far_copies + send(
                ((pass_side, far_side), (pass_main, far_main)),
                (far_sends, far_recvs),
                jump - 1,
                target,
            )
    for copy in far_copies:
        copy.wait()
    for made in pair_copies.values():
        for copy in made:
            copy.wait_send()
    for copy in near_copies.values():
        copy.wait_send()

    def last_side(side):
        row_scale = lax.rsqrt(side[:, square_column : square_column + 1] / width + EPS)
        rate_ref[...] = (side * row_scale).astype(rate_ref.dtype)
        return row_scale

    def last_main(span, total, row_scale):
        rows_ref[:, span] = (total * row_scale).astype(rows_ref.dtype)

    add_up(
        mine,
        1,
        [(pair_main, 0)] + [(far_main, jump) for jump in range(half - 1)],
        [(pair_side, 0)] + [(far_side, jump) for jump in range(half - 1)],
        last_side,
        last_main,
    )


def scatter_rows(part, side, width, square_column):
    ranks, rows, columns = part.shape
    side_columns = side.shape[2]
    near = inner_size(ranks)
    far = ranks // near
    vmem = pl.BlockSpec(memory_space=pltpu.VMEM)
    return pl.pallas_call(
        functools.partial(scatter_kernel, near, far, width, square_column),
        out_shape=(
            jax.ShapeDtypeStruct((rows, columns), jnp.bfloat16),
            jax.ShapeDtypeStruct((rows, side_columns), jnp.bfloat16),
        ),
        in_specs=[vmem, vmem],
        out_specs=(vmem, vmem),
        scratch_shapes=[
            pltpu.VMEM((far, near - 1, rows, columns), jnp.bfloat16),
            pltpu.VMEM((far, near - 1, rows, side_columns), jnp.bfloat16),
            pltpu.VMEM((far // 2, rows, columns), jnp.bfloat16),
            pltpu.VMEM((far // 2, rows, side_columns), jnp.bfloat16),
            pltpu.VMEM((far // 2, rows, columns), jnp.bfloat16),
            pltpu.VMEM((far // 2, rows, side_columns), jnp.bfloat16),
            pltpu.VMEM((far // 2 - 1, rows, columns), jnp.bfloat16),
            pltpu.VMEM((far // 2 - 1, rows, side_columns), jnp.bfloat16),
            pltpu.VMEM((far // 2 - 1, rows, columns), jnp.bfloat16),
            pltpu.VMEM((far // 2 - 1, rows, side_columns), jnp.bfloat16),
            pltpu.SemaphoreType.DMA((2, far, near - 1)),
            pltpu.SemaphoreType.DMA((2, far, near - 1)),
            pltpu.SemaphoreType.DMA((2, far // 2)),
            pltpu.SemaphoreType.DMA((2, far // 2)),
            pltpu.SemaphoreType.DMA((2, far // 2 - 1)),
            pltpu.SemaphoreType.DMA((2, far // 2 - 1)),
        ],
        compiler_params=pltpu.CompilerParams(collective_id=0, has_side_effects=True),
    )(part, side)


def out_kernel(
    ranks,
    blocks,
    gated_ref,
    w_ref,
    mixed_ref,
    gathered,
    terms,
    landed,
    gather_sends,
    gather_recvs,
    term_sends,
    term_recvs,
):
    mine = lax.axis_index("kv")
    column = lax.axis_index("tp")
    ratio = ranks // blocks
    owner = mine // ratio
    place = lax.rem(mine, ratio)
    slab = w_ref.shape[1]
    barrier = pltpu.get_barrier_semaphore()
    for offset in range(1, ranks):
        pl.semaphore_signal(
            barrier,
            inc=1,
            device_id=(lax.rem(mine + offset, ranks), column),
            device_id_type=MESH,
        )
    for near in range(ratio):
        source = column * ratio + near
        for block in range(blocks):

            @pl.when(block != column)
            def _():
                pl.semaphore_signal(
                    barrier, inc=1, device_id=(source, block), device_id_type=MESH
                )

    @pl.when(owner == column)
    def _():
        pl.semaphore_wait(barrier, ranks - 1)

    @pl.when(owner != column)
    def _():
        pl.semaphore_wait(barrier, 2 * ranks - 1)

    inner = inner_size(ranks)
    outer = ranks // inner
    my_outer = mine // inner
    my_inner = lax.rem(mine, inner)

    def spot(step_outer, step_inner):
        return lax.rem(my_outer + step_outer, outer) * inner + lax.rem(
            my_inner + step_inner, inner
        )

    copies = {}

    def gather_copy(source, offset, target):
        copy = pltpu.make_async_remote_copy(
            src_ref=source,
            dst_ref=gathered.at[offset - 1],
            send_sem=gather_sends.at[offset - 1],
            recv_sem=gather_recvs.at[offset - 1],
            device_id=(target, column),
            device_id_type=MESH,
        )
        copy.start()
        copies[offset] = copy

    for step in range(1, outer):
        gather_copy(gated_ref, step * inner, spot(step, 0))
    for step in range(1, inner):
        gather_copy(gated_ref, step, spot(0, step))

    def term_copy(offset, target):
        return pltpu.make_async_remote_copy(
            src_ref=terms.at[offset],
            dst_ref=landed.at[place, column],
            send_sem=term_sends.at[offset],
            recv_sem=term_recvs.at[place, column],
            device_id=(target, owner),
            device_id_type=MESH,
        )

    def origin(offset):
        return spot(outer - offset // inner, inner - offset % inner)

    turns = [0] + [step * inner for step in range(1, outer)]
    turns = turns + [offset for offset in range(ranks) if offset % inner]
    for offset in turns:
        target = origin(offset)
        if offset == 0:
            block = gated_ref[...]
        else:
            copies[offset].wait_recv()
            if offset % inner == 0:
                for step in range(1, inner):
                    gather_copy(gathered.at[offset - 1], offset + step, spot(0, step))
            block = gathered[offset - 1]
        term = jnp.dot(block, w_ref[...], preferred_element_type=jnp.float32).astype(
            jnp.bfloat16
        )
        if offset == 0:

            @pl.when(owner == column)
            def _():
                landed[place, column] = term

            @pl.when(owner != column)
            def _():
                terms[0] = term
                term_copy(0, target).start()

        else:
            terms[offset] = term
            term_copy(offset, target).start()

    for near in range(ratio):
        source = column * ratio + near
        for block in range(blocks):

            @pl.when(jnp.logical_or(source != mine, block != column))
            def _():
                pltpu.make_async_remote_copy(
                    src_ref=terms.at[0],
                    dst_ref=landed.at[near, block],
                    send_sem=term_sends.at[0],
                    recv_sem=term_recvs.at[near, block],
                    device_id=(source, block),
                    device_id_type=MESH,
                ).wait_recv()

        total = landed[near, 0].astype(jnp.float32)
        for block in range(1, blocks):
            total = total + landed[near, block].astype(jnp.float32)
        mixed_ref[:, near * slab : (near + 1) * slab] = total.astype(mixed_ref.dtype)
    for offset in range(ranks):
        target = origin(offset)
        if offset == 0:

            @pl.when(owner != column)
            def _():
                term_copy(0, target).wait_send()

        else:
            copies[offset].wait_send()
            term_copy(offset, target).wait_send()


def project_out(gated, w_out, ranks, blocks):
    rows = gated.shape[0]
    inner, slab = w_out.shape
    ratio = ranks // blocks
    vmem = pl.BlockSpec(memory_space=pltpu.VMEM)
    return pl.pallas_call(
        functools.partial(out_kernel, ranks, blocks),
        out_shape=jax.ShapeDtypeStruct((rows, ratio * slab), jnp.bfloat16),
        in_specs=[vmem, vmem],
        out_specs=vmem,
        scratch_shapes=[
            pltpu.VMEM((ranks - 1, rows, inner), jnp.bfloat16),
            pltpu.VMEM((ranks, rows, slab), jnp.bfloat16),
            pltpu.VMEM((ratio, blocks, rows, slab), jnp.bfloat16),
            pltpu.SemaphoreType.DMA((ranks - 1,)),
            pltpu.SemaphoreType.DMA((ranks - 1,)),
            pltpu.SemaphoreType.DMA((ranks,)),
            pltpu.SemaphoreType.DMA((ratio, blocks)),
        ],
        compiler_params=pltpu.CompilerParams(collective_id=1, has_side_effects=True),
    )(gated, w_out)


def conv_window(history, taps, amount):
    values = history.astype(jnp.float32)
    weights = taps.astype(jnp.float32)
    summed = weights[0] * values[:, 0:amount, :]
    for distance in range(1, weights.shape[0]):
        summed = summed + weights[distance] * values[:, distance : distance + amount, :]
    return jax.nn.silu(summed)


def commit_rows(history, accepted, keep):
    picked = accepted[:, None] + jnp.arange(keep, dtype=jnp.int32)[None, :]
    select = (
        picked[:, :, None] == jnp.arange(history.shape[1], dtype=jnp.int32)[None, None, :]
    ).astype(jnp.float32)
    return jnp.einsum("skl,slc->skc", select, history.astype(jnp.float32), precision=HIGH).astype(
        jnp.bfloat16
    )


def replay_state(
    state, history_x, history_b, path_dt, conv_wx, conv_wb, accepted, rate_bias, a_rate, per_group
):
    seq_count, heads, head_dim, state_dim = state.shape
    path_len = path_dt.shape[1]
    path_xs = conv_window(history_x, conv_wx, path_len).reshape(
        seq_count, path_len, heads, head_dim
    )
    path_bs = conv_window(history_b, conv_wb, path_len).reshape(
        seq_count, path_len, heads // per_group, state_dim
    )
    path_bh = jnp.repeat(path_bs, per_group, axis=2)
    path_step = jax.nn.softplus(path_dt.astype(jnp.float32) + rate_bias)
    is_live = (jnp.arange(path_len, dtype=jnp.int32)[None, :] < accepted[:, None]).astype(
        jnp.float32
    )[:, :, None]
    log_decay = path_step * a_rate * is_live
    overall = jnp.sum(log_decay, axis=1)
    tail_sum = overall[:, None, :] - jnp.cumsum(log_decay, axis=1)
    weights = is_live * jnp.exp(tail_sum) * path_step
    grown = jnp.einsum("sjh,sjhp,sjhn->shpn", weights, path_xs, path_bh, precision=HIGH)
    return jnp.exp(overall)[:, :, None, None] * state + grown


def tree_links(parents, keep):
    seq_count, prop_count = parents.shape
    front = jnp.broadcast_to(jnp.arange(-1, keep - 1, dtype=jnp.int32)[None, :], (seq_count, keep))
    parent_ids = jnp.concatenate([front, parents + keep], axis=1)
    nodes = keep + prop_count
    links = (parent_ids[:, :, None] == jnp.arange(nodes, dtype=jnp.int32)[None, None, :]).astype(
        jnp.float32
    )
    identity = jnp.eye(prop_count, dtype=jnp.float32)[None, :, :]
    ancestry = identity + links[:, keep:, keep:]
    for turn in range(prop_count.bit_length()):
        ancestry = jnp.minimum(jnp.einsum("sij,sjk->sik", ancestry, ancestry, precision=HIGH), 1.0)
    return (links, ancestry)


def tree_conv(buffer, rows, taps, links, keep):
    values = jnp.concatenate([buffer, rows], axis=1).astype(jnp.float32)
    weights = taps.astype(jnp.float32)
    last_tap = weights.shape[0] - 1
    summed = weights[last_tap] * values
    reached = values
    for distance in range(1, last_tap + 1):
        reached = jnp.einsum("sij,sjc->sic", links, reached, precision=HIGH)
        summed = summed + weights[last_tap - distance] * reached
    return jax.nn.silu(summed[:, keep:, :])


def tree_mix(
    state,
    post_x,
    post_b,
    post_c,
    rate_rows,
    z_rows,
    ancestry,
    rate_bias,
    a_rate,
    d_skip,
    gain_out,
    per_group,
):
    seq_count, prop_count, _ = post_x.shape
    heads, head_dim, state_dim = (state.shape[1], state.shape[2], state.shape[3])
    groups = heads // per_group
    x_heads = post_x.reshape(seq_count, prop_count, heads, head_dim)
    b_groups = post_b.reshape(seq_count, prop_count, groups, state_dim)
    c_groups = post_c.reshape(seq_count, prop_count, groups, state_dim)
    step_size = jax.nn.softplus(rate_rows.astype(jnp.float32) + rate_bias)
    path_decay = jnp.einsum("sij,sjh->sih", ancestry, step_size * a_rate, precision=HIGH)
    c_heads = jnp.repeat(c_groups, per_group, axis=2)
    carried = (
        jnp.einsum("sihn,shpn->sihp", c_heads, state, precision=HIGH)
        * jnp.exp(path_decay)[:, :, :, None]
    )
    scores = jnp.einsum("sign,sjgn->sgij", c_groups, b_groups, precision=HIGH)
    scores = jnp.repeat(scores, per_group, axis=1)
    decay_t = jnp.transpose(path_decay, (0, 2, 1))
    decay_gap = decay_t[:, :, :, None] - decay_t[:, :, None, :]
    is_live = ancestry[:, None, :, :] > 0.5
    mixing = jnp.where(is_live, jnp.exp(jnp.where(is_live, decay_gap, 0.0)), 0.0)
    mixing = mixing * jnp.transpose(step_size, (0, 2, 1))[:, :, None, :]
    within = jnp.einsum("shij,sjhp->sihp", scores * mixing, x_heads, precision=HIGH)
    heads_out = carried + within + d_skip[None, None, :, None] * x_heads
    heads_out = heads_out.reshape(seq_count, prop_count, heads * head_dim) * jax.nn.silu(
        z_rows.astype(jnp.float32)
    )
    grouped = heads_out.reshape(seq_count, prop_count, groups, per_group * head_dim)
    grouped = grouped * lax.rsqrt(jnp.mean(grouped * grouped, axis=-1, keepdims=True) + EPS)
    return (grouped.reshape(seq_count, prop_count, heads * head_dim) * gain_out).astype(
        jnp.bfloat16
    )


def shards(
    tokens,
    parents,
    accepted,
    state,
    conv_x,
    conv_b,
    conv_c,
    path_x,
    path_b,
    path_c,
    path_dt,
    gain_in,
    w_x,
    w_z,
    w_b,
    w_c,
    w_dt,
    dt_bias,
    a_log,
    d_skip,
    conv_wx,
    conv_wb,
    conv_wc,
    gain_out,
    w_out,
):
    seq_local = state.shape[0]
    proposals = parents.shape[1]
    heads_local = dt_bias.shape[0]
    inner_local = w_x.shape[1]
    group_cols = w_b.shape[1]
    width = gain_in.shape[0]
    keep = conv_wx.shape[0] - 1
    tp_index = lax.axis_index("tp")
    kv_index = lax.axis_index("kv")
    slab_width = tokens.shape[2]
    flat_rows = tokens.reshape(-1, slab_width).astype(jnp.float32)
    gain_part = lax.dynamic_slice_in_dim(gain_in, kv_index * slab_width, slab_width)
    scaled = (flat_rows * gain_part).astype(jnp.bfloat16)
    w_joined = jnp.concatenate([w_x, w_z, w_b, w_c], axis=1)
    ranks = lax.axis_size("kv")
    blocks = lax.axis_size("tp")
    part = jnp.dot(scaled, w_joined, preferred_element_type=jnp.float32).astype(jnp.bfloat16)
    w_rate = lax.dynamic_slice(
        w_dt, (kv_index * slab_width, tp_index * heads_local), (slab_width, heads_local)
    )
    rate_term = jnp.dot(scaled, w_rate, preferred_element_type=jnp.float32)
    squares = jnp.sum(flat_rows * flat_rows, axis=1, keepdims=True)
    side = jnp.concatenate([rate_term, squares], axis=1).astype(jnp.bfloat16)
    side = jnp.pad(side, ((0, 0), (0, -side.shape[1] % 128)))
    rows_all, rate_all = scatter_rows(
        part.reshape(ranks, -1, part.shape[1]),
        side.reshape(ranks, -1, side.shape[1]),
        width,
        heads_local,
    )

    def column_part(lower, upper):
        return rows_all[:, lower:upper].reshape(seq_local, proposals, upper - lower)

    x_rows = column_part(0, inner_local)
    z_rows = column_part(inner_local, 2 * inner_local)
    b_rows = column_part(2 * inner_local, 2 * inner_local + group_cols)
    c_rows = column_part(2 * inner_local + group_cols, 2 * inner_local + 2 * group_cols)
    rate_rows = rate_all[:, :heads_local].reshape(seq_local, proposals, heads_local)
    a_rate = -jnp.exp(a_log)
    history_x = jnp.concatenate([conv_x, path_x], axis=1)
    history_b = jnp.concatenate([conv_b, path_b], axis=1)
    history_c = jnp.concatenate([conv_c, path_c], axis=1)
    new_state = replay_state(
        state, history_x, history_b, path_dt, conv_wx, conv_wb, accepted, dt_bias, a_rate, HPG
    )
    links, ancestry = tree_links(parents, keep)
    post_x = tree_conv(commit_rows(history_x, accepted, keep), x_rows, conv_wx, links, keep)
    post_b = tree_conv(commit_rows(history_b, accepted, keep), b_rows, conv_wb, links, keep)
    post_c = tree_conv(commit_rows(history_c, accepted, keep), c_rows, conv_wc, links, keep)
    gated = tree_mix(
        new_state,
        post_x,
        post_b,
        post_c,
        rate_rows,
        z_rows,
        ancestry,
        dt_bias,
        a_rate,
        d_skip,
        gain_out,
        HPG,
    )
    gated_flat = gated.reshape(-1, inner_local)
    summed = project_out(gated_flat, w_out, ranks, blocks)
    mixed = summed.reshape(seq_local, proposals, -1)
    return (mixed, new_state)


def solution(mesh):
    return jax.shard_map(
        shards,
        mesh=mesh,
        in_specs=(
            P(None, None, "kv"),
            P("kv", None),
            P("kv"),
            P("kv", "tp", None, None),
            P("kv", None, "tp"),
            P("kv", None, "tp"),
            P("kv", None, "tp"),
            P("kv", None, "tp"),
            P("kv", None, "tp"),
            P("kv", None, "tp"),
            P("kv", None, "tp"),
            P(),
            P("kv", "tp"),
            P("kv", "tp"),
            P("kv", "tp"),
            P("kv", "tp"),
            P(),
            P("tp"),
            P("tp"),
            P("tp"),
            P(None, "tp"),
            P(None, "tp"),
            P(None, "tp"),
            P("tp"),
            P("tp", "kv"),
        ),
        out_specs=(P("kv", None, "tp"), P("kv", "tp", None, None)),
        check_vma=False,
    )
```

```python
import functools

import jax
import jax.numpy as jnp
from jax import lax
from jax.experimental import pallas as pl
from jax.experimental.pallas import tpu as pltpu
from jax.sharding import PartitionSpec as P

HPG = 4


EPS = 1e-06
HIGH = lax.Precision.HIGHEST
MESH = pl.DeviceIdType.MESH


def inner_size(ranks):
    return max(d for d in range(1, ranks + 1) if ranks % d == 0 and d * d <= ranks)


def scatter_kernel(
    near,
    far,
    width,
    square_column,
    part_ref,
    side_ref,
    rows_ref,
    rate_ref,
    near_main,
    near_side,
    sum_main,
    sum_side,
    pair_main,
    pair_side,
    pass_main,
    pass_side,
    far_main,
    far_side,
    near_sends,
    near_recvs,
    pair_sends,
    pair_recvs,
    far_sends,
    far_recvs,
):
    mine = lax.axis_index("kv")
    column = lax.axis_index("tp")
    my_far = mine // near
    my_near = lax.rem(mine, near)
    partner = my_far + 1 - 2 * lax.rem(my_far, 2)
    half = far // 2

    def place(home, jump, step_near):
        return lax.rem(home + 2 * jump, far) * near + lax.rem(my_near + step_near, near)

    barrier = pltpu.get_barrier_semaphore()
    peers = [place(my_far, 0, step) for step in range(1, near)]
    peers = peers + [place(partner, 0, 0)]
    peers = peers + [place(my_far, jump, 0) for jump in range(1, half)]
    for peer in peers:
        pl.semaphore_signal(barrier, inc=1, device_id=(peer, column), device_id_type=MESH)
    pl.semaphore_wait(barrier, len(peers))

    order = [(jump, kind) for jump in list(range(1, half)) + [0] for kind in range(2)]
    homes = (partner, my_far)
    near_copies = {}

    def start_near(jump, kind):
        slot = 2 * jump + kind
        for step in range(1, near):
            for which, (source, landing) in enumerate(
                ((side_ref, near_side), (part_ref, near_main))
            ):
                copy = pltpu.make_async_remote_copy(
                    src_ref=source.at[place(homes[kind], jump, step)],
                    dst_ref=landing.at[slot, step - 1],
                    send_sem=near_sends.at[which, slot, step - 1],
                    recv_sem=near_recvs.at[which, slot, step - 1],
                    device_id=(place(my_far, 0, step), column),
                    device_id_type=MESH,
                )
                copy.start()
                near_copies[slot, step, which] = copy

    start_near(*order[0])
    columns = rows_ref.shape[1]
    chunk = 512 if columns % 512 == 0 else columns

    def add_up(block, slot, extra_main, extra_side, put_side, put_main):
        side = side_ref[block].astype(jnp.float32)
        for step in range(1, near):
            side = side + near_side[slot, step - 1].astype(jnp.float32)
        for ref, place_of in extra_side:
            side = side + ref[place_of].astype(jnp.float32)
        state = put_side(side)

        @pl.loop(0, columns // chunk)
        def _(turn):
            span = pl.ds(pl.multiple_of(turn * chunk, chunk), chunk)
            total = part_ref[block, :, span].astype(jnp.float32)
            for step in range(1, near):
                total = total + near_main[slot, step - 1, :, span].astype(jnp.float32)
            for ref, place_of in extra_main:
                total = total + ref[place_of, :, span].astype(jnp.float32)
            put_main(span, total, state)

    def send(refs, sems, source_at, target):
        made = []
        for which, (source, landing) in enumerate(refs):
            copy = pltpu.make_async_remote_copy(
                src_ref=source.at[source_at],
                dst_ref=landing.at[source_at],
                send_sem=sems[0].at[which, source_at],
                recv_sem=sems[1].at[which, source_at],
                device_id=(target, column),
                device_id_type=MESH,
            )
            copy.start()
            made.append(copy)
        return made

    def keep_side(ref, at):
        def put(side):
            ref[at] = side.astype(ref.dtype)

        return put

    def keep_main(ref, at):
        def put(span, total, state):
            ref[at, :, span] = total.astype(ref.dtype)

        return put

    pair_copies = {}
    far_copies = []
    for turn, (jump, kind) in enumerate(order):
        slot = 2 * jump + kind
        for step in range(1, near):
            for which in range(2):
                near_copies[slot, step, which].wait_recv()
        if turn + 1 < len(order):
            start_near(*order[turn + 1])
        if kind == 0:
            add_up(
                place(partner, jump, 0),
                slot,
                [],
                [],
                keep_side(sum_side, jump),
                keep_main(sum_main, jump),
            )
            pair_copies[jump] = send(
                ((sum_side, pair_side), (sum_main, pair_main)),
                (pair_sends, pair_recvs),
                jump,
                place(partner, 0, 0),
            )
            continue
        for copy in pair_copies[jump]:
            copy.wait_recv()
        if jump > 0:
            target = place(my_far, jump, 0)
            add_up(
                target,
                slot,
                [(pair_main, jump)],
                [(pair_side, jump)],
                keep_side(pass_side, jump - 1),
                keep_main(pass_main, jump - 1),
            )
            far_copies = far_copies + send(
                ((pass_side, far_side), (pass_main, far_main)),
                (far_sends, far_recvs),
                jump - 1,
                target,
            )
    for copy in far_copies:
        copy.wait()
    for made in pair_copies.values():
        for copy in made:
            copy.wait_send()
    for copy in near_copies.values():
        copy.wait_send()

    def last_side(side):
        row_scale = lax.rsqrt(side[:, square_column : square_column + 1] / width + EPS)
        rate_ref[...] = (side * row_scale).astype(rate_ref.dtype)
        return row_scale

    def last_main(span, total, row_scale):
        rows_ref[:, span] = (total * row_scale).astype(rows_ref.dtype)

    add_up(
        mine,
        1,
        [(pair_main, 0)] + [(far_main, jump) for jump in range(half - 1)],
        [(pair_side, 0)] + [(far_side, jump) for jump in range(half - 1)],
        last_side,
        last_main,
    )


def scatter_rows(part, side, width, square_column):
    ranks, rows, columns = part.shape
    side_columns = side.shape[2]
    near = inner_size(ranks)
    far = ranks // near
    vmem = pl.BlockSpec(memory_space=pltpu.VMEM)
    return pl.pallas_call(
        functools.partial(scatter_kernel, near, far, width, square_column),
        out_shape=(
            jax.ShapeDtypeStruct((rows, columns), jnp.bfloat16),
            jax.ShapeDtypeStruct((rows, side_columns), jnp.bfloat16),
        ),
        in_specs=[vmem, vmem],
        out_specs=(vmem, vmem),
        scratch_shapes=[
            pltpu.VMEM((far, near - 1, rows, columns), jnp.bfloat16),
            pltpu.VMEM((far, near - 1, rows, side_columns), jnp.bfloat16),
            pltpu.VMEM((far // 2, rows, columns), jnp.bfloat16),
            pltpu.VMEM((far // 2, rows, side_columns), jnp.bfloat16),
            pltpu.VMEM((far // 2, rows, columns), jnp.bfloat16),
            pltpu.VMEM((far // 2, rows, side_columns), jnp.bfloat16),
            pltpu.VMEM((far // 2 - 1, rows, columns), jnp.bfloat16),
            pltpu.VMEM((far // 2 - 1, rows, side_columns), jnp.bfloat16),
            pltpu.VMEM((far // 2 - 1, rows, columns), jnp.bfloat16),
            pltpu.VMEM((far // 2 - 1, rows, side_columns), jnp.bfloat16),
            pltpu.SemaphoreType.DMA((2, far, near - 1)),
            pltpu.SemaphoreType.DMA((2, far, near - 1)),
            pltpu.SemaphoreType.DMA((2, far // 2)),
            pltpu.SemaphoreType.DMA((2, far // 2)),
            pltpu.SemaphoreType.DMA((2, far // 2 - 1)),
            pltpu.SemaphoreType.DMA((2, far // 2 - 1)),
        ],
        compiler_params=pltpu.CompilerParams(collective_id=0, has_side_effects=True),
    )(part, side)


def out_kernel(
    ranks,
    blocks,
    gated_ref,
    w_ref,
    mixed_ref,
    gathered,
    terms,
    landed,
    gather_sends,
    gather_recvs,
    term_sends,
    term_recvs,
):
    mine = lax.axis_index("kv")
    column = lax.axis_index("tp")
    ratio = ranks // blocks
    owner = mine // ratio
    place = lax.rem(mine, ratio)
    slab = w_ref.shape[1]
    barrier = pltpu.get_barrier_semaphore()
    for offset in range(1, ranks):
        pl.semaphore_signal(
            barrier,
            inc=1,
            device_id=(lax.rem(mine + offset, ranks), column),
            device_id_type=MESH,
        )
    for near in range(ratio):
        source = column * ratio + near
        for block in range(blocks):

            @pl.when(block != column)
            def _():
                pl.semaphore_signal(
                    barrier, inc=1, device_id=(source, block), device_id_type=MESH
                )

    @pl.when(owner == column)
    def _():
        pl.semaphore_wait(barrier, ranks - 1)

    @pl.when(owner != column)
    def _():
        pl.semaphore_wait(barrier, 2 * ranks - 1)

    inner = inner_size(ranks)
    outer = ranks // inner
    my_outer = mine // inner
    my_inner = lax.rem(mine, inner)

    def spot(step_outer, step_inner):
        return lax.rem(my_outer + step_outer, outer) * inner + lax.rem(
            my_inner + step_inner, inner
        )

    copies = {}

    def gather_copy(source, offset, target):
        copy = pltpu.make_async_remote_copy(
            src_ref=source,
            dst_ref=gathered.at[offset - 1],
            send_sem=gather_sends.at[offset - 1],
            recv_sem=gather_recvs.at[offset - 1],
            device_id=(target, column),
            device_id_type=MESH,
        )
        copy.start()
        copies[offset] = copy

    for step in range(1, outer):
        gather_copy(gated_ref, step * inner, spot(step, 0))
    for step in range(1, inner):
        gather_copy(gated_ref, step, spot(0, step))

    def term_copy(offset, target):
        return pltpu.make_async_remote_copy(
            src_ref=terms.at[offset],
            dst_ref=landed.at[place, column],
            send_sem=term_sends.at[offset],
            recv_sem=term_recvs.at[place, column],
            device_id=(target, owner),
            device_id_type=MESH,
        )

    def origin(offset):
        return spot(outer - offset // inner, inner - offset % inner)

    turns = [0] + [step * inner for step in range(1, outer)]
    turns = turns + [offset for offset in range(ranks) if offset % inner]
    for offset in turns:
        target = origin(offset)
        if offset == 0:
            block = gated_ref[...]
        else:
            copies[offset].wait_recv()
            if offset % inner == 0:
                for step in range(1, inner):
                    gather_copy(gathered.at[offset - 1], offset + step, spot(0, step))
            block = gathered[offset - 1]
        term = jnp.dot(block, w_ref[...], preferred_element_type=jnp.float32).astype(
            jnp.bfloat16
        )
        if offset == 0:

            @pl.when(owner == column)
            def _():
                landed[place, column] = term

            @pl.when(owner != column)
            def _():
                terms[0] = term
                term_copy(0, target).start()

        else:
            terms[offset] = term
            term_copy(offset, target).start()

    for near in range(ratio):
        source = column * ratio + near
        for block in range(blocks):

            @pl.when(jnp.logical_or(source != mine, block != column))
            def _():
                pltpu.make_async_remote_copy(
                    src_ref=terms.at[0],
                    dst_ref=landed.at[near, block],
                    send_sem=term_sends.at[0],
                    recv_sem=term_recvs.at[near, block],
                    device_id=(source, block),
                    device_id_type=MESH,
                ).wait_recv()

        total = landed[near, 0].astype(jnp.float32)
        for block in range(1, blocks):
            total = total + landed[near, block].astype(jnp.float32)
        mixed_ref[:, near * slab : (near + 1) * slab] = total.astype(mixed_ref.dtype)
    for offset in range(ranks):
        target = origin(offset)
        if offset == 0:

            @pl.when(owner != column)
            def _():
                term_copy(0, target).wait_send()

        else:
            copies[offset].wait_send()
            term_copy(offset, target).wait_send()


def project_out(gated, w_out, ranks, blocks):
    rows = gated.shape[0]
    inner, slab = w_out.shape
    ratio = ranks // blocks
    vmem = pl.BlockSpec(memory_space=pltpu.VMEM)
    return pl.pallas_call(
        functools.partial(out_kernel, ranks, blocks),
        out_shape=jax.ShapeDtypeStruct((rows, ratio * slab), jnp.bfloat16),
        in_specs=[vmem, vmem],
        out_specs=vmem,
        scratch_shapes=[
            pltpu.VMEM((ranks - 1, rows, inner), jnp.bfloat16),
            pltpu.VMEM((ranks, rows, slab), jnp.bfloat16),
            pltpu.VMEM((ratio, blocks, rows, slab), jnp.bfloat16),
            pltpu.SemaphoreType.DMA((ranks - 1,)),
            pltpu.SemaphoreType.DMA((ranks - 1,)),
            pltpu.SemaphoreType.DMA((ranks,)),
            pltpu.SemaphoreType.DMA((ratio, blocks)),
        ],
        compiler_params=pltpu.CompilerParams(collective_id=1, has_side_effects=True),
    )(gated, w_out)


def conv_window(history, taps, amount):
    values = history.astype(jnp.float32)
    weights = taps.astype(jnp.float32)
    summed = weights[0] * values[:, 0:amount, :]
    for distance in range(1, weights.shape[0]):
        summed = summed + weights[distance] * values[:, distance : distance + amount, :]
    return jax.nn.silu(summed)


def commit_rows(history, accepted, keep):
    picked = accepted[:, None] + jnp.arange(keep, dtype=jnp.int32)[None, :]
    select = (
        picked[:, :, None] == jnp.arange(history.shape[1], dtype=jnp.int32)[None, None, :]
    ).astype(jnp.float32)
    return jnp.einsum("skl,slc->skc", select, history.astype(jnp.float32), precision=HIGH).astype(
        jnp.bfloat16
    )


def replay_state(
    state, history_x, history_b, path_dt, conv_wx, conv_wb, accepted, rate_bias, a_rate, per_group
):
    seq_count, heads, head_dim, state_dim = state.shape
    path_len = path_dt.shape[1]
    path_xs = conv_window(history_x, conv_wx, path_len).reshape(
        seq_count, path_len, heads, head_dim
    )
    path_bs = conv_window(history_b, conv_wb, path_len).reshape(
        seq_count, path_len, heads // per_group, state_dim
    )
    path_bh = jnp.repeat(path_bs, per_group, axis=2)
    path_step = jax.nn.softplus(path_dt.astype(jnp.float32) + rate_bias)
    is_live = (jnp.arange(path_len, dtype=jnp.int32)[None, :] < accepted[:, None]).astype(
        jnp.float32
    )[:, :, None]
    log_decay = path_step * a_rate * is_live
    overall = jnp.sum(log_decay, axis=1)
    tail_sum = overall[:, None, :] - jnp.cumsum(log_decay, axis=1)
    weights = is_live * jnp.exp(tail_sum) * path_step
    grown = jnp.einsum("sjh,sjhp,sjhn->shpn", weights, path_xs, path_bh, precision=HIGH)
    return jnp.exp(overall)[:, :, None, None] * state + grown


def tree_links(parents, keep):
    seq_count, prop_count = parents.shape
    front = jnp.broadcast_to(jnp.arange(-1, keep - 1, dtype=jnp.int32)[None, :], (seq_count, keep))
    parent_ids = jnp.concatenate([front, parents + keep], axis=1)
    nodes = keep + prop_count
    links = (parent_ids[:, :, None] == jnp.arange(nodes, dtype=jnp.int32)[None, None, :]).astype(
        jnp.float32
    )
    identity = jnp.eye(prop_count, dtype=jnp.float32)[None, :, :]
    ancestry = identity + links[:, keep:, keep:]
    for turn in range(prop_count.bit_length()):
        ancestry = jnp.minimum(jnp.einsum("sij,sjk->sik", ancestry, ancestry, precision=HIGH), 1.0)
    return (links, ancestry)


def tree_conv(buffer, rows, taps, links, keep):
    values = jnp.concatenate([buffer, rows], axis=1).astype(jnp.float32)
    weights = taps.astype(jnp.float32)
    last_tap = weights.shape[0] - 1
    summed = weights[last_tap] * values
    reached = values
    for distance in range(1, last_tap + 1):
        reached = jnp.einsum("sij,sjc->sic", links, reached, precision=HIGH)
        summed = summed + weights[last_tap - distance] * reached
    return jax.nn.silu(summed[:, keep:, :])


def tree_mix(
    state,
    post_x,
    post_b,
    post_c,
    rate_rows,
    z_rows,
    ancestry,
    rate_bias,
    a_rate,
    d_skip,
    gain_out,
    per_group,
):
    seq_count, prop_count, _ = post_x.shape
    heads, head_dim, state_dim = (state.shape[1], state.shape[2], state.shape[3])
    groups = heads // per_group
    x_heads = post_x.reshape(seq_count, prop_count, heads, head_dim)
    b_groups = post_b.reshape(seq_count, prop_count, groups, state_dim)
    c_groups = post_c.reshape(seq_count, prop_count, groups, state_dim)
    step_size = jax.nn.softplus(rate_rows.astype(jnp.float32) + rate_bias)
    path_decay = jnp.einsum("sij,sjh->sih", ancestry, step_size * a_rate, precision=HIGH)
    c_heads = jnp.repeat(c_groups, per_group, axis=2)
    carried = (
        jnp.einsum("sihn,shpn->sihp", c_heads, state, precision=HIGH)
        * jnp.exp(path_decay)[:, :, :, None]
    )
    scores = jnp.einsum("sign,sjgn->sgij", c_groups, b_groups, precision=HIGH)
    scores = jnp.repeat(scores, per_group, axis=1)
    decay_t = jnp.transpose(path_decay, (0, 2, 1))
    decay_gap = decay_t[:, :, :, None] - decay_t[:, :, None, :]
    is_live = ancestry[:, None, :, :] > 0.5
    mixing = jnp.where(is_live, jnp.exp(jnp.where(is_live, decay_gap, 0.0)), 0.0)
    mixing = mixing * jnp.transpose(step_size, (0, 2, 1))[:, :, None, :]
    within = jnp.einsum("shij,sjhp->sihp", scores * mixing, x_heads, precision=HIGH)
    heads_out = carried + within + d_skip[None, None, :, None] * x_heads
    heads_out = heads_out.reshape(seq_count, prop_count, heads * head_dim) * jax.nn.silu(
        z_rows.astype(jnp.float32)
    )
    grouped = heads_out.reshape(seq_count, prop_count, groups, per_group * head_dim)
    grouped = grouped * lax.rsqrt(jnp.mean(grouped * grouped, axis=-1, keepdims=True) + EPS)
    return (grouped.reshape(seq_count, prop_count, heads * head_dim) * gain_out).astype(
        jnp.bfloat16
    )


def shards(
    tokens,
    parents,
    accepted,
    state,
    conv_x,
    conv_b,
    conv_c,
    path_x,
    path_b,
    path_c,
    path_dt,
    gain_in,
    w_x,
    w_z,
    w_b,
    w_c,
    w_dt,
    dt_bias,
    a_log,
    d_skip,
    conv_wx,
    conv_wb,
    conv_wc,
    gain_out,
    w_out,
):
    seq_local = state.shape[0]
    proposals = parents.shape[1]
    heads_local = dt_bias.shape[0]
    inner_local = w_x.shape[1]
    group_cols = w_b.shape[1]
    width = gain_in.shape[0]
    keep = conv_wx.shape[0] - 1
    tp_index = lax.axis_index("tp")
    kv_index = lax.axis_index("kv")
    slab_width = tokens.shape[2]
    flat_rows = tokens.reshape(-1, slab_width).astype(jnp.float32)
    gain_part = lax.dynamic_slice_in_dim(gain_in, kv_index * slab_width, slab_width)
    scaled = (flat_rows * gain_part).astype(jnp.bfloat16)
    w_joined = jnp.concatenate([w_x, w_z, w_b, w_c], axis=1)
    ranks = lax.axis_size("kv")
    blocks = lax.axis_size("tp")
    part = jnp.dot(scaled, w_joined, preferred_element_type=jnp.float32).astype(jnp.bfloat16)
    w_rate = lax.dynamic_slice(
        w_dt, (kv_index * slab_width, tp_index * heads_local), (slab_width, heads_local)
    )
    rate_term = jnp.dot(scaled, w_rate, preferred_element_type=jnp.float32)
    squares = jnp.sum(flat_rows * flat_rows, axis=1, keepdims=True)
    side = jnp.concatenate([rate_term, squares], axis=1).astype(jnp.bfloat16)
    side = jnp.pad(side, ((0, 0), (0, -side.shape[1] % 128)))
    rows_all, rate_all = scatter_rows(
        part.reshape(ranks, -1, part.shape[1]),
        side.reshape(ranks, -1, side.shape[1]),
        width,
        heads_local,
    )

    def column_part(lower, upper):
        return rows_all[:, lower:upper].reshape(seq_local, proposals, upper - lower)

    x_rows = column_part(0, inner_local)
    z_rows = column_part(inner_local, 2 * inner_local)
    b_rows = column_part(2 * inner_local, 2 * inner_local + group_cols)
    c_rows = column_part(2 * inner_local + group_cols, 2 * inner_local + 2 * group_cols)
    rate_rows = rate_all[:, :heads_local].reshape(seq_local, proposals, heads_local)
    a_rate = -jnp.exp(a_log)
    history_x = jnp.concatenate([conv_x, path_x], axis=1)
    history_b = jnp.concatenate([conv_b, path_b], axis=1)
    history_c = jnp.concatenate([conv_c, path_c], axis=1)
    new_state = replay_state(
        state, history_x, history_b, path_dt, conv_wx, conv_wb, accepted, dt_bias, a_rate, HPG
    )
    links, ancestry = tree_links(parents, keep)
    post_x = tree_conv(commit_rows(history_x, accepted, keep), x_rows, conv_wx, links, keep)
    post_b = tree_conv(commit_rows(history_b, accepted, keep), b_rows, conv_wb, links, keep)
    post_c = tree_conv(commit_rows(history_c, accepted, keep), c_rows, conv_wc, links, keep)
    gated = tree_mix(
        new_state,
        post_x,
        post_b,
        post_c,
        rate_rows,
        z_rows,
        ancestry,
        dt_bias,
        a_rate,
        d_skip,
        gain_out,
        HPG,
    )
    gated_flat = gated.reshape(-1, inner_local)
    summed = project_out(gated_flat, w_out, ranks, blocks)
    mixed = summed.reshape(seq_local, proposals, -1)
    return (mixed, new_state)


def solution(mesh):
    return jax.shard_map(
        shards,
        mesh=mesh,
        in_specs=(
            P(None, None, "kv"),
            P("kv", None),
            P("kv"),
            P("kv", "tp", None, None),
            P("kv", None, "tp"),
            P("kv", None, "tp"),
            P("kv", None, "tp"),
            P("kv", None, "tp"),
            P("kv", None, "tp"),
            P("kv", None, "tp"),
            P("kv", None, "tp"),
            P(),
            P("kv", "tp"),
            P("kv", "tp"),
            P("kv", "tp"),
            P("kv", "tp"),
            P(),
            P("tp"),
            P("tp"),
            P("tp"),
            P(None, "tp"),
            P(None, "tp"),
            P(None, "tp"),
            P("tp"),
            P("tp", "kv"),
        ),
        out_specs=(P("kv", None, "tp"), P("kv", "tp", None, None)),
        check_vma=False,
    )
```
